512 devices in a mesh: sp: 32 (over z, x), tp: 16 (over y, core).
Axes of the slice: x: 4, y: 8, z: 8, core: 2. Of those that a mesh axis runs over, the one named last changes fastest.
Arguments:
- queries: bfloat16 [8192, 1536], P('sp', 'tp'), may hold values from -500 to 500
- latent: bfloat16 [8192, 256], P('sp'), may hold values from -6 to 6
- rope_key: bfloat16 [8192, 32], P('sp'), may hold values from -6 to 6
- latent_gain: bfloat16 [256], replicated, may hold values from 0.099609375 to 1.8984375
- key_value_weight: bfloat16 [256, 2048], P(None, 'tp'), may hold values from -0.375 to 0.375
- out_weight: bfloat16 [1024, 2048], P(None, 'tp'), may hold values from -6 to 6
- residual: bfloat16 [8192, 2048], P('sp', 'tp'), may hold values from -150 to 150
- ffn_gain: bfloat16 [2048], replicated, may hold values from 0.099609375 to 1.8984375
- routes: int32 [8192, 2], P('sp'), may hold values from 0 to 31, all different within a row; in each aligned block of 256 rows (0 to 255, 256 to 511, ...) at most 32 rows name the same one
- route_prob: float32 [8192, 2], P('sp'), may hold values from 0.1 to 1
- group_weight: float32 [8192], P('sp'), may hold values from 0.25 to 1
- gate_weight: bfloat16 [32, 2048, 4096], P('sp', None, 'tp'), may hold values from -0.125 to 0.125
- up_weight: bfloat16 [32, 2048, 4096], P('sp', None, 'tp'), may hold values from -0.125 to 0.125
- down_weight: bfloat16 [32, 4096, 2048], P('sp', None, 'tp'), may hold values from -0.75 to 0.75
Outputs:
- final: bfloat16 [8192, 2048], P('sp', 'tp')
The draws below stay inside these ranges and needn't reach their ends.
Inputs may be any that keep to these rules, and one draw needn't show every extreme that they name: `routes`: each row names 2 different experts; among the 256 rows of one index of sp no expert is named more than 32 times, a bound that some block reaches.
All inputs are finite; a program needn't handle non-finite values.
Results may differ from the reference program's by a relative error of at most 0.015.
The reference program's roundings to bfloat16 on the way count: a program that leaves them out, or rounds other values in their place, can miss the bound.
Values may be sent and summed in bfloat16 or wider, within the bound.
No kernel may reach another device: no remote copies, remote signals or barrier semaphores. Data moves between devices by JAX's collectives and lax.ppermute only.
A program may use at most 64 MiB of HBM per device.

```python
import math
import jax
import jax.numpy as jnp
import numpy as np
from jax import lax

D = 2048
HEADS = 16
NOPE = 64
ROPE = 32
VDIM = 64
RANK = 256
FF = 4096
TOP = 2
SPAN = 64
TOK_SP = 256
TOKENS = 8192
EXPERTS = 32
CAP = 32
N_SP = 32


def draw_residual(key, part):
    keys = jax.random.split(jax.random.fold_in(key, 11), 3)
    base = jnp.clip(jax.random.normal(keys[0], (TOKENS, D), jnp.float32), -6.0, 6.0)
    column = jnp.exp(math.log(4.0) * jnp.arange(D, dtype=jnp.float32) / D)
    column = column * jax.random.uniform(keys[1], (D,), jnp.float32, 0.7, 1.3)
    rows = jnp.exp(jax.random.uniform(keys[2], (TOKENS, 1), jnp.float32, math.log(0.5), math.log(2.0)))
    return (base * rows * column[None, :]).astype(jnp.bfloat16)


def draw_queries(key, part):
    keys = jax.random.split(jax.random.fold_in(key, 23), 1)
    base = jnp.clip(jax.random.normal(keys[0], (TOKENS, HEADS * (NOPE + ROPE)), jnp.float32), -6.0, 6.0)
    return base.astype(jnp.bfloat16)


def block_scale(own_key, extent, pieces, least, largest):
    def one(axis_at, shards_of):
        heights = jax.random.uniform(jax.random.fold_in(jax.random.fold_in(own_key, 6), axis_at), (shards_of,), jnp.float32, least / len(pieces), largest / len(pieces))
        return jnp.repeat(jnp.exp(heights), extent[axis_at] // shards_of).reshape((-1,) + (1,) * (len(extent) - axis_at - 1))

    level = one(*pieces[0])
    for cut in pieces[1:]:
        level = level * one(*cut)
    return level


def shared_out(own_key, own, number, rows, count, top, bound, lean):
    order = jax.random.permutation(own_key, count)
    crowded, usual = portions_of(count, rows * top, bound, lean, True), portions_of(count, rows * top, bound, lean, False)
    places = jnp.arange(count)

    def named(lengths, offset_by):
        used = int((lengths > 0).sum())
        fixed = max(1, used // 4)
        moved = fixed + (places - fixed + offset_by * (used - fixed)) % max(1, count - fixed)
        return jnp.zeros((count,), jnp.int32).at[order[jnp.where(places < fixed, places, moved)]].set(jnp.asarray(lengths, jnp.int32))

    lengths = jnp.where(number % 4 == 0, named(crowded, number // 4), named(usual, number - number // 4 - 1))
    mixed = jax.random.permutation(jax.random.fold_in(own, 3), count)
    donor, receiver = mixed[0:count // 2 * 2:2], mixed[1:count // 2 * 2:2]
    slack = jnp.minimum(lengths[donor] - 1, bound - lengths[receiver]) // 2
    slack = jnp.where((donor == order[0]) | (receiver == order[0]) | (lengths[receiver] == 0), 0, jnp.maximum(slack, 0))
    moved = jax.random.randint(jax.random.fold_in(own, 4), (count // 2,), 0, 1 << 20) % (slack + 1)
    lengths = lengths.at[donor].add(-moved).at[receiver].add(moved)
    members = jnp.searchsorted(jnp.cumsum(lengths), jnp.arange(rows * top), side="right").astype(jnp.int32)
    table = members.reshape(top, rows).T
    table = table[jax.random.permutation(jax.random.fold_in(own, 1), rows)]
    offset_by = jax.random.randint(jax.random.fold_in(own, 2), (rows, 1), 0, top)
    return jnp.take_along_axis(table, (jnp.arange(top)[None, :] + offset_by) % top, axis=1)


def portions_of(amount, total, reach, slope, full):
    portions = [(1 << 20) // math.isqrt(grade ** slope) + 1 for grade in range(1, amount + 1)]
    largest = reach if full else min(reach, max(-(-total // amount), total * portions[0] // sum(portions)))
    least = 1 if total - largest >= amount - 1 else 0
    counts, spare = [largest] + [least] * (amount - 1), total - largest - least * (amount - 1)
    while spare > 0:
        movable = [i for i in range(1, amount) if counts[i] < largest] or [i for i in range(1, amount) if counts[i] < reach]
        mass, budget = sum([portions[i] for i in movable]), spare
        for i in movable:
            more = min(reach - counts[i], max(1, budget * portions[i] // mass), spare)
            counts[i] = counts[i] + more
            spare = spare - more
    return np.array(counts)


def normal_values(own_key, extent, spread, bound, cuts=(), kind=jnp.bfloat16):
    array = jax.random.normal(own_key, extent, jnp.float32) * spread
    if len(cuts) > 0:
        array = block_scale(own_key, extent, cuts, -0.22, 0.18) * array
    return jnp.clip(array, min=-bound, max=bound).astype(kind)


def setup_inputs(seed: int = 0) -> dict:
    splits = jax.random.split(jax.random.key(seed), 15)
    queries = draw_queries(jax.random.fold_in(splits[14], 71), 0)
    latent = normal_values(splits[1], (TOKENS, RANK), 1.0, 6.0, ((0, 32),))
    rope_key = normal_values(splits[2], (TOKENS, ROPE), 1.0, 6.0, ((0, 32),))
    latent_gain = jnp.clip(1.0 + 0.18 * jax.random.normal(splits[3], (RANK,), jnp.float32), 0.099609375, 1.8984375).astype(jnp.bfloat16)
    key_value_weight = normal_values(splits[4], (RANK, HEADS * (NOPE + VDIM)), RANK ** -0.5, 0.375, ((1, 16),))
    out_weight = normal_values(splits[5], (HEADS * VDIM, D), 1.0, 6.0, ((1, 16),))
    residual = draw_residual(jax.random.fold_in(splits[14], 71), 0)
    ffn_gain = jnp.clip(1.0 + 0.18 * jax.random.normal(splits[7], (D,), jnp.float32), 0.099609375, 1.8984375).astype(jnp.bfloat16)
    routes_keys = jax.random.split(jax.random.fold_in(splits[8], 1), TOKENS // TOK_SP)
    routes_turns = jax.random.permutation(jax.random.fold_in(splits[8], 3), TOKENS // TOK_SP)
    routes = jax.vmap(lambda own, number: shared_out(jax.random.fold_in(splits[8], 2), own, number, TOK_SP, EXPERTS, TOP, CAP, 1))(routes_keys, routes_turns).reshape((TOKENS, TOP))
    route_prob = jnp.clip(jnp.exp(math.log(1.0) - 2.3025851 * jax.random.uniform(splits[9], (TOKENS, TOP), jnp.float32) ** block_scale(splits[9], (TOKENS, TOP), ((0, 32),), -0.2, 0.2)), 0.1, 1.0)
    group_weight = jnp.clip(0.25 + 0.75 * jax.random.uniform(splits[10], (TOKENS,), jnp.float32) ** block_scale(splits[10], (TOKENS,), ((0, 32),), -0.2, 0.2), 0.25, 1.0)
    gate_weight = normal_values(splits[11], (EXPERTS, D, FF), D ** -0.5, 0.125, ((0, 32), (2, 16)))
    up_weight = normal_values(splits[12], (EXPERTS, D, FF), D ** -0.5, 0.125, ((0, 32), (2, 16)))
    down_weight = normal_values(splits[13], (EXPERTS, FF, D), (FF // 64) ** -0.5, 0.75, ((0, 32), (2, 16)))
    return {"queries": queries, "latent": latent, "rope_key": rope_key, "latent_gain": latent_gain, "key_value_weight": key_value_weight, "out_weight": out_weight, "residual": residual, "ffn_gain": ffn_gain, "routes": routes, "route_prob": route_prob, "group_weight": group_weight, "gate_weight": gate_weight, "up_weight": up_weight, "down_weight": down_weight}


THETA = 500000.0
EPSILON = 1e-06

def rotate(values, positions):
    rot_width = values.shape[-1]
    half_width = rot_width // 2
    frequency = 1.0 / THETA ** (jnp.arange(0, rot_width, 2, dtype=jnp.float32) / rot_width)
    angles = positions.astype(jnp.float32)[:, None] * frequency[None, :]
    view_shape = (values.shape[0],) + (1,) * (values.ndim - 2) + (half_width,)
    cos_table = jnp.cos(angles).reshape(view_shape)
    sin_table = jnp.sin(angles).reshape(view_shape)
    wide = values.astype(jnp.float32)
    lower_half = wide[..., :half_width]
    upper_half = wide[..., half_width:]
    return jnp.concatenate([lower_half * cos_table - upper_half * sin_table, upper_half * cos_table + lower_half * sin_table], axis=-1)

def reference(queries, latent, rope_key, latent_gain, key_value_weight, out_weight, residual, ffn_gain, routes, route_prob, group_weight, gate_weight, up_weight, down_weight):
    count = queries.shape[0]
    positions = jnp.arange(count, dtype=jnp.int32)
    query = queries.reshape(count, HEADS, NOPE + ROPE)
    query = jnp.concatenate([query[..., :NOPE].astype(jnp.float32), rotate(query[..., NOPE:], positions)], axis=-1).astype(jnp.bfloat16)
    latent_wide = latent.astype(jnp.float32)
    normed = latent_wide * lax.rsqrt(lax.optimization_barrier(jnp.mean(latent_wide * latent_wide, axis=-1, keepdims=True)) + EPSILON)
    normed = (normed * latent_gain.astype(jnp.float32)).astype(jnp.bfloat16)
    key_value = jnp.dot(normed, key_value_weight, preferred_element_type=jnp.float32).astype(jnp.bfloat16).reshape(count, HEADS, NOPE + VDIM)
    rotated = rotate(rope_key, positions).astype(jnp.bfloat16)
    key_nope = key_value[..., :NOPE].astype(jnp.float32)
    values = key_value[..., NOPE:].astype(jnp.float32)
    rotated_wide = rotated.astype(jnp.float32)
    key_blocks = positions // SPAN
    query_block = math.gcd(count, 512)
    scaling = (NOPE + ROPE) ** (-0.5)

    def one_block(block_index):
        first_row = (block_index * query_block).astype(jnp.int32)
        part = lax.dynamic_slice_in_dim(query, first_row, query_block, 0).astype(jnp.float32)
        scores = jnp.einsum('qhd,khd->hqk', part[..., :NOPE], key_nope)
        scores = scores + jnp.einsum('qhd,kd->hqk', part[..., NOPE:], rotated_wide)
        scores = scores * scaling
        query_blocks = (first_row + jnp.arange(query_block, dtype=jnp.int32)) // SPAN
        allowed = key_blocks[None, :] <= query_blocks[:, None]
        scores = jnp.where(allowed[None, :, :], scores, -jnp.inf)
        row_max = lax.optimization_barrier(jnp.max(scores, axis=-1, keepdims=True))
        expd = jnp.exp(scores - row_max)
        denom = lax.optimization_barrier(jnp.sum(expd, axis=-1))
        weights_half = expd.astype(jnp.bfloat16).astype(jnp.float32)
        summed = jnp.einsum('hqk,khd->qhd', weights_half, values)
        return (summed / jnp.transpose(denom)[..., None]).astype(jnp.bfloat16)
    attended = lax.map(one_block, jnp.arange(count // query_block, dtype=jnp.int32)).reshape(count, HEADS * VDIM)
    mixed = (residual.astype(jnp.float32) + jnp.dot(attended, out_weight, preferred_element_type=jnp.float32)).astype(jnp.bfloat16)
    mixed_wide = mixed.astype(jnp.float32)
    row_scale = lax.rsqrt(lax.optimization_barrier(jnp.mean(mixed_wide * mixed_wide, axis=-1)) + EPSILON)
    scaled = (mixed_wide * ffn_gain.astype(jnp.float32)).astype(jnp.bfloat16)
    picks = routes.reshape(N_SP, TOK_SP * TOP)
    onehot = (picks[:, :, None] == jnp.arange(EXPERTS, dtype=jnp.int32)[None, None, :]).astype(jnp.int32)
    slot_index = lax.optimization_barrier(jnp.sum((jnp.cumsum(onehot, axis=1) - 1) * onehot, axis=2))
    group_index = jnp.arange(N_SP, dtype=jnp.int32)[:, None]
    target = (picks * (N_SP * CAP) + group_index * CAP + slot_index).reshape(-1).astype(jnp.int32)
    token_of = jnp.arange(count * TOP, dtype=jnp.int32) // TOP
    buffer = jnp.zeros((EXPERTS * N_SP * CAP, D), jnp.bfloat16).at[target].set(scaled[token_of])
    scale_buffer = jnp.zeros((EXPERTS * N_SP * CAP,), jnp.float32).at[target].set(row_scale[token_of])

    def run_expert(operands):
        rows, scales, gate_one, up_one, down_one = operands
        gate_acc = scales[:, None] * jnp.dot(rows, gate_one, preferred_element_type=jnp.float32)
        up_acc = scales[:, None] * jnp.dot(rows, up_one, preferred_element_type=jnp.float32)
        hidden = (jax.nn.silu(gate_acc) * up_acc).astype(jnp.bfloat16)
        return jnp.dot(hidden, down_one, preferred_element_type=jnp.float32).astype(jnp.bfloat16)
    expert_out = lax.map(run_expert, (buffer.reshape(EXPERTS, N_SP * CAP, D), scale_buffer.reshape(EXPERTS, N_SP * CAP), gate_weight, up_weight, down_weight))
    picked = expert_out.reshape(EXPERTS * N_SP * CAP, D)[target].astype(jnp.float32).reshape(count, TOP, D)
    combine = group_weight[:, None] * route_prob / lax.optimization_barrier(jnp.sum(route_prob, axis=-1, keepdims=True))
    routed_sum = lax.optimization_barrier(jnp.sum(combine[..., None] * picked, axis=1))
    return (mixed_wide + routed_sum).astype(jnp.bfloat16)
```

```python
import jax
import jax.numpy as jnp
from jax import lax
from jax.sharding import PartitionSpec as P

D = 2048
NOPE = 64
ROPE = 32
VDIM = 64
TOP = 2
SPAN = 64
X = 4
Z = 8
Y = 8
SP = X * Z
TP = Y * 2

THETA = 500000.0
EPSILON = 1e-06


def permute(value, target):
    pairs = []
    for s in range(SP):
        for t in range(TP):
            z, x, y, c = target(s // X, s % X, t // 2, t % 2)
            pairs.append((s * TP + t, ((z % Z) * X + x % X) * TP + (y % Y) * 2 + c))
    return lax.ppermute(value, ("sp", "tp"), pairs)


def side(core):
    return 1 - 2 * core


def swap(value):
    return permute(value, lambda z, x, y, c: (z, x, y, 1 - c))


def z_step(value):
    return permute(value, lambda z, x, y, c: (z + side(c), x, y, c))


def y_step(value):
    return permute(value, lambda z, x, y, c: (z, x, y + side(c), c))


def x_shift(value, by):
    return permute(value, lambda z, x, y, c: (z, x + by, y, c))


def tables(positions):
    half_width = ROPE // 2
    frequency = 1.0 / THETA ** (jnp.arange(0, ROPE, 2, dtype=jnp.float32) / ROPE)
    angles = positions.astype(jnp.float32)[:, None] * frequency[None, :]
    return jnp.cos(angles), jnp.sin(angles)


def rotate(values, positions):
    half_width = ROPE // 2
    cos_table, sin_table = tables(positions)
    wide = values.astype(jnp.float32)
    lower_half = wide[:, :half_width]
    upper_half = wide[:, half_width:]
    return jnp.concatenate(
        [
            lower_half * cos_table - upper_half * sin_table,
            upper_half * cos_table + lower_half * sin_table,
        ],
        axis=-1,
    ).astype(jnp.bfloat16)


def body(
    queries,
    latent,
    rope_key,
    latent_gain,
    key_value_weight,
    out_weight,
    residual,
    ffn_gain,
    routes,
    route_prob,
    group_weight,
    gate_weight,
    up_weight,
    down_weight,
):
    tokens = queries.shape[0]
    width = residual.shape[1]
    ff = gate_weight.shape[2]
    sp = lax.axis_index("sp")
    tp = lax.axis_index("tp")
    z, x = sp // X, sp % X
    y, core = tp // 2, tp % 2
    sign = 1 - 2 * core
    bf16, f32 = jnp.bfloat16, jnp.float32
    local = jnp.arange(tokens, dtype=jnp.int32)

    block = jnp.concatenate([latent, rope_key.T], axis=0)
    near = [z_step(block)]
    query = jnp.concatenate(
        [queries[:, :NOPE], rotate(queries[:, NOPE:], sp * tokens + local)], axis=1
    )
    query_parts = [query] + [x_shift(query, by) for by in range(1, X)]
    for _ in range(3):
        near.append(z_step(near[-1]))
    far = [swap(one) for one in near[:3]]

    down = down_weight.reshape(TP, ff, width)

    def down_rows(chip, first):
        base = (chip % Y) * 2
        pick = lambda half: lax.dynamic_index_in_dim(down, base + half, 0, keepdims=False)
        return jnp.concatenate([pick(first), pick(1 - first)], axis=0)

    down_parts = []
    for k in range(1, 5):
        same = permute(
            down_rows(y - sign * k, core), lambda zz, xx, yy, c: (zz, xx, yy - side(c) * k, c)
        )
        other = permute(
            down_rows(y + sign * k, 1 - core),
            lambda zz, xx, yy, c: (zz, xx, yy + side(c) * k, 1 - c),
        )
        down_parts.append(jnp.concatenate([same, other], axis=1))
    down_own = down_rows(y, core)

    gate = gate_weight.reshape(TP, width, ff)
    up = up_weight.reshape(TP, width, ff)
    gains = ffn_gain.astype(f32).reshape(TP, width)

    def feature_rows(chip, first):
        base = (chip % Y) * 2
        parts, scales = [], []
        for half in (first, 1 - first):
            pick = lambda a: lax.dynamic_index_in_dim(a, base + half, 0, keepdims=False)
            parts.append(jnp.concatenate([pick(gate), pick(up)], axis=1))
            scales.append(pick(gains))
        return jnp.concatenate(parts, axis=0), jnp.concatenate(scales, axis=0)

    experts = SP
    capacity = 2 * tokens * TOP // experts
    slots = experts * capacity
    named = jnp.arange(experts, dtype=jnp.int32)[None, :]
    one_hot = [(routes[:, k : k + 1] == named).astype(f32) for k in range(TOP)]
    both = (one_hot[0] + one_hot[1]).astype(bf16)
    earlier = (local[None, :] < local[:, None]).astype(bf16)
    before = jnp.dot(earlier, both, preferred_element_type=f32)
    targets = []
    for k in range(TOP):
        rank = jnp.sum(before * one_hot[k], axis=1).astype(jnp.int32)
        targets.append(routes[:, k] * capacity + rank)
    slot_row = jnp.arange(slots, dtype=jnp.int32)
    select = [(targets[k][:, None] == slot_row[None, :]).astype(bf16) for k in range(TOP)]
    placed = select[0] + select[1]

    column = [z] + [z - sign * k for k in range(1, 5)] + [z + sign * k for k in range(1, 4)]
    column = jnp.stack([one % Z for one in column])
    blocks = jnp.stack([block] + near + far)
    latent_wide = blocks[:, :tokens].astype(f32)
    normed = latent_wide * lax.rsqrt(
        jnp.mean(latent_wide * latent_wide, axis=-1, keepdims=True) + EPSILON
    )
    normed = (normed * latent_gain.astype(f32)).astype(bf16).reshape(Z * tokens, -1)
    key_value = jnp.dot(normed, key_value_weight, preferred_element_type=f32).astype(bf16)
    key_positions = ((column * X + x) * tokens)[:, None] + local[None, :]
    rope_all = jnp.transpose(blocks[:, tokens:], (0, 2, 1)).reshape(Z * tokens, ROPE)
    rotated = rotate(rope_all, key_positions.reshape(-1))
    keys = jnp.concatenate([key_value[:, :NOPE], rotated], axis=1)
    query_all = jnp.concatenate(query_parts, axis=0)
    scores = lax.dot_general(keys, query_all, (((1,), (1,)), ((), ())), preferred_element_type=f32)
    scores = scores * (NOPE + ROPE) ** (-0.5)
    query_starts = jnp.stack([(z * X + (x - i) % X) * tokens for i in range(X)])
    query_blocks = ((query_starts[:, None] + local[None, :]) // SPAN).reshape(-1)
    key_blocks = (key_positions // SPAN).reshape(-1)
    allowed = key_blocks[:, None] <= query_blocks[None, :]
    scores = jnp.where(allowed, scores, -jnp.inf)
    top = jnp.maximum(jnp.max(scores, axis=0, keepdims=True), -1e30)
    expd = jnp.exp(scores - top)
    total = jnp.sum(expd, axis=0, keepdims=True)
    summed = lax.dot_general(
        key_value[:, NOPE:], expd.astype(bf16), (((0,), (0,)), ((), ())), preferred_element_type=f32
    )
    packed = jnp.concatenate([summed, top, total, jnp.zeros((6, X * tokens), f32)], axis=0)
    packed = [packed[:, i * tokens : (i + 1) * tokens] for i in range(X)]
    packed = [packed[0]] + [x_shift(packed[i], -i) for i in range(1, X)]
    tops = [one[VDIM : VDIM + 1] for one in packed]
    top_all = jnp.maximum(jnp.maximum(tops[0], tops[1]), jnp.maximum(tops[2], tops[3]))
    factors = [jnp.exp(one - top_all) for one in tops]
    merged = sum(factors[i] * packed[i] for i in range(X))
    attended = (merged[:VDIM] / merged[VDIM + 1 : VDIM + 2]).astype(bf16)

    attended_all = lax.all_gather(attended, "tp", axis=0, tiled=True)
    projected = lax.dot_general(
        attended_all, out_weight, (((0,), (0,)), ((), ())), preferred_element_type=f32
    )
    mixed = (residual.astype(f32) + projected).astype(bf16)

    sent = lax.dot_general(placed, mixed, (((0,), (0,)), ((), ())), preferred_element_type=f32)
    sent = sent.astype(bf16).reshape(SP, capacity, width)
    arrived = lax.all_to_all(sent, "sp", split_axis=0, concat_axis=0, tiled=True)
    arrived = arrived.reshape(slots, width)

    def products(rows, weights):
        weight, gain = weights
        wide = rows.astype(f32)
        scaled = (wide * gain[None, :]).astype(bf16)
        return jnp.dot(scaled, weight, preferred_element_type=f32), jnp.sum(
            wide * wide, axis=1, keepdims=True
        )

    chip = jnp.concatenate([arrived, swap(arrived)], axis=1)
    gate_up, squares = products(chip, feature_rows(y, core))
    passing = chip
    for k in range(1, 5):
        passing = y_step(passing)
        more, more_squares = products(passing, feature_rows(y - sign * k, core))
        gate_up, squares = gate_up + more, squares + more_squares
        if k < 4:
            more, more_squares = products(swap(passing), feature_rows(y + sign * k, 1 - core))
            gate_up, squares = gate_up + more, squares + more_squares
    row_scale = lax.rsqrt(squares / D + EPSILON)
    gate_full = gate_up[:, :ff] * row_scale
    up_full = gate_up[:, ff:] * row_scale
    hidden = (jax.nn.silu(gate_full) * up_full).astype(bf16)

    hidden = jnp.concatenate([hidden, swap(hidden)], axis=1)
    half = slots // 2
    start = lax.dynamic_slice_in_dim(hidden, core * half, half, 0)
    passing = jnp.dot(start, down_parts[3], preferred_element_type=f32).astype(bf16)
    passing = y_step(passing)
    mine = (jnp.arange(slots, dtype=jnp.int32) // half == core)[:, None]
    passing = jnp.where(mine, jnp.concatenate([passing, passing], axis=0).astype(f32), 0.0)
    for k in (3, 2, 1):
        passing = passing + jnp.dot(hidden, down_parts[k - 1], preferred_element_type=f32)
        passing = y_step(passing.astype(bf16)).astype(f32)
    crossed = swap(passing[:, width:].astype(bf16)).astype(f32)
    expert_out = jnp.dot(hidden, down_own, preferred_element_type=f32)
    expert_out = (expert_out + passing[:, :width] + crossed).astype(bf16)

    returned = lax.all_to_all(
        expert_out.reshape(SP, capacity, width), "sp", split_axis=0, concat_axis=0, tiled=True
    ).reshape(slots, width)
    combine = group_weight[:, None] * route_prob / jnp.sum(route_prob, axis=-1, keepdims=True)
    final = mixed.astype(f32)
    for k in range(TOP):
        picked = jnp.dot(select[k], returned, preferred_element_type=f32)
        final = final + combine[:, k : k + 1] * picked
    return final.astype(bf16)


def solution(mesh):
    return jax.shard_map(
        body,
        mesh=mesh,
        in_specs=(
            P("sp", "tp"),
            P("sp", None),
            P("sp", None),
            P(),
            P(None, "tp"),
            P(None, "tp"),
            P("sp", "tp"),
            P(),
            P("sp", None),
            P("sp", None),
            P("sp"),
            P("sp", None, "tp"),
            P("sp", None, "tp"),
            P("sp", None, "tp"),
        ),
        out_specs=P("sp", "tp"),
        check_vma=False,
    )
```

```python
import jax
import jax.numpy as jnp
from jax import lax
from jax.sharding import PartitionSpec as P

D = 2048
NOPE = 64
ROPE = 32
VDIM = 64
TOP = 2
SPAN = 64
X = 4
Z = 8
Y = 8
SP = X * Z
TP = Y * 2

THETA = 500000.0
EPSILON = 1e-06

EARLY = (4, 1, 7, 2)
LATE = (6, 3, 5)


Z_GROUPS = [[z * X + x for z in range(Z)] for x in range(X)]
X_GROUPS = [[z * X + x for x in range(X)] for z in range(Z)]


def exchange(value, axis, groups=None):
    return lax.all_to_all(
        value, axis, split_axis=0, concat_axis=0, tiled=True, axis_index_groups=groups
    )


def swap(value):
    return lax.ppermute(value, "tp", [(t, t ^ 1) for t in range(TP)])


def x_shift(value, by):
    return lax.ppermute(
        value, "sp", [(s, s // X * X + (s + by) % X) for s in range(SP)]
    )


def y_step(value, by):
    return lax.ppermute(value, "tp", [(t, (t + 2 * by) % TP) for t in range(TP)])


def tables(positions):
    frequency = 1.0 / THETA ** (jnp.arange(0, ROPE, 2, dtype=jnp.float32) / ROPE)
    angles = positions.astype(jnp.float32)[:, None] * frequency[None, :]
    return jnp.cos(angles), jnp.sin(angles)


def rotate(values, positions):
    half_width = ROPE // 2
    cos_table, sin_table = tables(positions)
    wide = values.astype(jnp.float32)
    lower_half = wide[:, :half_width]
    upper_half = wide[:, half_width:]
    return jnp.concatenate(
        [
            lower_half * cos_table - upper_half * sin_table,
            upper_half * cos_table + lower_half * sin_table,
        ],
        axis=-1,
    ).astype(jnp.bfloat16)


def body(
    queries,
    latent,
    rope_key,
    latent_gain,
    key_value_weight,
    out_weight,
    residual,
    ffn_gain,
    routes,
    route_prob,
    group_weight,
    gate_weight,
    up_weight,
    down_weight,
):
    tokens = queries.shape[0]
    width = residual.shape[1]
    ff = gate_weight.shape[2]
    sp = lax.axis_index("sp")
    tp = lax.axis_index("tp")
    z, x = sp // X, sp % X
    y, core = tp // 2, tp % 2
    bf16, f32 = jnp.bfloat16, jnp.float32
    local = jnp.arange(tokens, dtype=jnp.int32)

    latent_wide = latent.astype(f32)
    normed = latent_wide * lax.rsqrt(
        jnp.mean(latent_wide * latent_wide, axis=-1, keepdims=True) + EPSILON
    )
    normed = (normed * latent_gain.astype(f32)).astype(bf16)
    key_value = lax.dot_general(
        key_value_weight, normed, (((0,), (1,)), ((), ())), preferred_element_type=f32
    ).astype(bf16)
    positions = sp * tokens + local
    rotated = rotate(rope_key, positions).T
    block = jnp.concatenate([key_value[:NOPE], rotated, key_value[NOPE:]], axis=0)
    query = jnp.concatenate([queries[:, :NOPE], rotate(queries[:, NOPE:], positions)], axis=1)
    copies, query = lax.optimization_barrier(
        (jnp.broadcast_to(block, (Z,) + block.shape), query)
    )
    blocks = exchange(copies, "sp", Z_GROUPS)

    query_parts = [query]
    for by in range(1, X):
        query_parts.append(x_shift(query, by))
    query_parts = jnp.stack(query_parts)
    at = lambda a, chip: lax.dynamic_index_in_dim(a, chip, 0, keepdims=False)
    query_all = jnp.concatenate([at(query_parts, (x - one) % X) for one in range(X)], axis=0)

    gate_up_weight = jnp.concatenate(
        [gate_weight.reshape(TP, width, ff), up_weight.reshape(TP, width, ff)], axis=2
    )
    gains = ffn_gain.astype(f32).reshape(TP, width)
    down = down_weight.reshape(Y, 2, ff, width)
    down = jnp.where(core == 0, down, down[:, ::-1]).reshape(Y, 2 * ff, width)
    down_parts = {0: at(down, y)}
    for by in EARLY:
        down_parts[by] = y_step(at(down, (y + by) % Y), by)
    late = {by: at(down, (y + by) % Y) for by in LATE}

    experts = SP
    capacity = 2 * tokens * TOP // experts
    slots = experts * capacity
    named = jnp.arange(experts, dtype=jnp.int32)[None, :]
    one_hot = [(routes[:, k : k + 1] == named).astype(f32) for k in range(TOP)]
    both = (one_hot[0] + one_hot[1]).astype(bf16)
    earlier = (local[None, :] < local[:, None]).astype(bf16)
    before = jnp.dot(earlier, both, preferred_element_type=f32)
    slot_row = jnp.arange(slots, dtype=jnp.int32)
    select = []
    for k in range(TOP):
        rank = jnp.sum(before * one_hot[k], axis=1).astype(jnp.int32)
        slot = routes[:, k] * capacity + rank
        select.append((slot[:, None] == slot_row[None, :]).astype(bf16))
    placed = select[0] + select[1]

    scores = jnp.einsum(
        "zdk,qd->zkq", blocks[:, : NOPE + ROPE], query_all, preferred_element_type=f32
    )
    scores = scores * (NOPE + ROPE) ** (-0.5)
    query_positions = z * X * tokens + jnp.arange(X * tokens, dtype=jnp.int32)
    key_starts = (jnp.arange(Z, dtype=jnp.int32) * X + x) * tokens
    key_blocks = (key_starts[:, None] + local[None, :]) // SPAN
    allowed = key_blocks[:, :, None] <= (query_positions // SPAN)[None, None, :]
    scores = jnp.where(allowed, scores, -jnp.inf)
    top = jnp.maximum(jnp.max(scores, axis=(0, 1)), -1e30)[None, :]
    expd = jnp.exp(scores - top[None])
    total = jnp.sum(expd, axis=(0, 1))[None, :]
    summed = jnp.einsum(
        "zvk,zkq->vq", blocks[:, NOPE + ROPE :], expd.astype(bf16), preferred_element_type=f32
    )
    packed = jnp.concatenate([summed, top, total, jnp.zeros((6, X * tokens), f32)], axis=0)
    packed = jnp.stack([packed[:, i * tokens : (i + 1) * tokens] for i in range(X)])
    packed = exchange(packed, "sp", X_GROUPS)
    tops = packed[:, VDIM]
    factors = jnp.exp(tops - jnp.max(tops, axis=0, keepdims=True))
    merged = jnp.sum(factors[:, None, :] * packed, axis=0)
    attended = (merged[:VDIM] / merged[VDIM + 1 : VDIM + 2]).astype(bf16)
    attended, gate_up_weight, down_parts, placed = lax.optimization_barrier(
        (attended, gate_up_weight, down_parts, placed)
    )

    attended_all = lax.all_gather(attended, "tp", axis=0, tiled=True)
    projected = lax.dot_general(
        attended_all, out_weight, (((0,), (0,)), ((), ())), preferred_element_type=f32
    )
    mixed = (residual.astype(f32) + projected).astype(bf16)

    sent = lax.dot_general(placed, mixed, (((0,), (0,)), ((), ())), preferred_element_type=f32)
    sent, late = lax.optimization_barrier((sent.astype(bf16), late))
    arrived = exchange(sent.reshape(SP, capacity, width), "sp").reshape(slots, width)
    for by in LATE:
        late[by] = y_step(late[by], by)
    arrived, late = lax.optimization_barrier((arrived, late))
    down_parts = {**down_parts, **late}

    def products(parts):
        scaled, weights, squares = [], [], 0.0
        for rows, chip, side in parts:
            wide = rows.astype(f32)
            device = (chip % Y) * 2 + side
            scaled.append((wide * at(gains, device)[None, :]).astype(bf16))
            weights.append(at(gate_up_weight, device))
            squares = squares + jnp.sum(wide * wide, axis=1, keepdims=True)
        product = jnp.dot(
            jnp.concatenate(scaled, axis=1),
            jnp.concatenate(weights, axis=0),
            preferred_element_type=f32,
        )
        return product, squares

    half = slots // 2

    def ring(above, below):
        above = y_step(above, 1)
        below = y_step(below, -1)
        return above, below

    above = below = arrived
    gate_up, squares = products([(arrived, y, core), (swap(arrived), y, 1 - core)])
    for k in range(1, 4):
        above, below = ring(above, below)
        crossed = swap(jnp.concatenate([above, below], axis=1))
        more, more_squares = products(
            [
                (above, y - k, core),
                (below, y + k, core),
                (crossed[:, :width], y - k, 1 - core),
                (crossed[:, width:], y + k, 1 - core),
            ]
        )
        gate_up, squares = gate_up + more, squares + more_squares
    last = jnp.concatenate(ring(above[:half], below[half:]), axis=0)
    more, more_squares = products([(last, y + 4, core), (swap(last), y + 4, 1 - core)])
    gate_up, squares = gate_up + more, squares + more_squares
    gate_up = gate_up * lax.rsqrt(squares / D + EPSILON)
    hidden = (jax.nn.silu(gate_up[:, :ff]) * gate_up[:, ff:]).astype(bf16)

    hidden = jnp.concatenate([hidden, swap(hidden)], axis=1)
    first = jnp.dot(hidden, down_parts[4], preferred_element_type=f32).astype(bf16)
    order = (3, 5, 2, 6, 1, 7, 0)
    rest = jnp.dot(
        hidden,
        jnp.concatenate([down_parts[by] for by in order], axis=1),
        preferred_element_type=f32,
    )
    rest = lax.optimization_barrier(rest)
    own = {by: rest[:, i * width : (i + 1) * width] for i, by in enumerate(order)}
    nothing = jnp.zeros((half, width), bf16)
    above = jnp.concatenate([y_step(first[:half], 1), nothing], axis=0)
    below = jnp.concatenate([nothing, y_step(first[half:], -1)], axis=0)
    for k in (3, 2, 1):
        above = y_step((above.astype(f32) + own[Y - k]).astype(bf16), 1)
        below = y_step((below.astype(f32) + own[k]).astype(bf16), -1)
    expert_out = own[0] + above.astype(f32) + below.astype(f32)
    expert_out = expert_out.astype(bf16).reshape(SP, capacity, width)

    returned = exchange(expert_out, "sp").reshape(slots, width)
    combine = group_weight[:, None] * route_prob / jnp.sum(route_prob, axis=-1, keepdims=True)
    final = mixed.astype(f32)
    for k in range(TOP):
        picked = jnp.dot(select[k], returned, preferred_element_type=f32)
        final = final + combine[:, k : k + 1] * picked
    return final.astype(bf16)


def solution(mesh):
    return jax.shard_map(
        body,
        mesh=mesh,
        in_specs=(
            P("sp", "tp"),
            P("sp", None),
            P("sp", None),
            P(),
            P(None, "tp"),
            P(None, "tp"),
            P("sp", "tp"),
            P(),
            P("sp", None),
            P("sp", None),
            P("sp"),
            P("sp", None, "tp"),
            P("sp", None, "tp"),
            P("sp", None, "tp"),
        ),
        out_specs=P("sp", "tp"),
        check_vma=False,
    )
```

```python
import jax
import jax.numpy as jnp
from jax import lax
from jax.sharding import PartitionSpec as P

D = 2048
NOPE = 64
ROPE = 32
VDIM = 64
TOP = 2
SPAN = 64
X = 4
Z = 8
Y = 8
SP = X * Z
TP = Y * 2

THETA = 500000.0
EPSILON = 1e-06


Z_GROUPS = [[z * X + x for z in range(Z)] for x in range(X)]
X_GROUPS = [[z * X + x for x in range(X)] for z in range(Z)]
Y_GROUPS = [[y * 2 + c for y in range(Y)] for c in range(2)]


def exchange(value, axis, groups=None):
    return lax.all_to_all(
        value, axis, split_axis=0, concat_axis=0, tiled=True, axis_index_groups=groups
    )


def swap(value):
    return lax.ppermute(value, "tp", [(t, t ^ 1) for t in range(TP)])


def x_shift(value, by):
    return lax.ppermute(
        value, "sp", [(s, s // X * X + (s + by) % X) for s in range(SP)]
    )


def y_step(value, by):
    return lax.ppermute(value, "tp", [(t, (t + 2 * by) % TP) for t in range(TP)])


def tables(positions):
    frequency = 1.0 / THETA ** (jnp.arange(0, ROPE, 2, dtype=jnp.float32) / ROPE)
    angles = positions.astype(jnp.float32)[:, None] * frequency[None, :]
    return jnp.cos(angles), jnp.sin(angles)


def rotate(values, positions):
    half_width = ROPE // 2
    cos_table, sin_table = tables(positions)
    wide = values.astype(jnp.float32)
    lower_half = wide[:, :half_width]
    upper_half = wide[:, half_width:]
    return jnp.concatenate(
        [
            lower_half * cos_table - upper_half * sin_table,
            upper_half * cos_table + lower_half * sin_table,
        ],
        axis=-1,
    ).astype(jnp.bfloat16)


def body(
    queries,
    latent,
    rope_key,
    latent_gain,
    key_value_weight,
    out_weight,
    residual,
    ffn_gain,
    routes,
    route_prob,
    group_weight,
    gate_weight,
    up_weight,
    down_weight,
):
    tokens = queries.shape[0]
    width = residual.shape[1]
    ff = gate_weight.shape[2]
    sp = lax.axis_index("sp")
    tp = lax.axis_index("tp")
    z, x = sp // X, sp % X
    y, core = tp // 2, tp % 2
    bf16, f32 = jnp.bfloat16, jnp.float32
    local = jnp.arange(tokens, dtype=jnp.int32)

    latent_wide = latent.astype(f32)
    normed = latent_wide * lax.rsqrt(
        jnp.mean(latent_wide * latent_wide, axis=-1, keepdims=True) + EPSILON
    )
    normed = (normed * latent_gain.astype(f32)).astype(bf16)
    key_value = lax.dot_general(
        key_value_weight, normed, (((0,), (1,)), ((), ())), preferred_element_type=f32
    ).astype(bf16)
    positions = sp * tokens + local
    rotated = rotate(rope_key, positions).T
    block = jnp.concatenate([key_value[:NOPE], rotated, key_value[NOPE:]], axis=0)
    query = jnp.concatenate([queries[:, :NOPE], rotate(queries[:, NOPE:], positions)], axis=1)
    blocks = lax.all_gather(block, "sp", axis=0, tiled=False, axis_index_groups=Z_GROUPS)

    query_parts = [query]
    for by in range(1, X):
        query_parts.append(x_shift(query, by))
    query_parts = jnp.stack(query_parts)
    at = lambda a, chip: lax.dynamic_index_in_dim(a, chip, 0, keepdims=False)
    query_all = jnp.concatenate([at(query_parts, (x - one) % X) for one in range(X)], axis=0)

    gate_up_weight = jnp.concatenate(
        [gate_weight.reshape(TP, width, ff), up_weight.reshape(TP, width, ff)], axis=2
    )
    gains = ffn_gain.astype(f32).reshape(TP, width)
    down = exchange(down_weight.reshape(Y, 2 * ff, width), "tp", Y_GROUPS)

    experts = SP
    capacity = 2 * tokens * TOP // experts
    slots = experts * capacity
    named = jnp.arange(experts, dtype=jnp.int32)[None, :]
    one_hot = [(routes[:, k : k + 1] == named).astype(f32) for k in range(TOP)]
    both = (one_hot[0] + one_hot[1]).astype(bf16)
    earlier = (local[None, :] < local[:, None]).astype(bf16)
    before = jnp.dot(earlier, both, preferred_element_type=f32)
    slot_row = jnp.arange(slots, dtype=jnp.int32)
    select = []
    for k in range(TOP):
        rank = jnp.sum(before * one_hot[k], axis=1).astype(jnp.int32)
        slot = routes[:, k] * capacity + rank
        select.append((slot[:, None] == slot_row[None, :]).astype(bf16))
    placed = select[0] + select[1]

    scores = jnp.einsum(
        "zdk,qd->zkq", blocks[:, : NOPE + ROPE], query_all, preferred_element_type=f32
    )
    scores = scores * (NOPE + ROPE) ** (-0.5)
    query_positions = z * X * tokens + jnp.arange(X * tokens, dtype=jnp.int32)
    key_starts = (jnp.arange(Z, dtype=jnp.int32) * X + x) * tokens
    key_blocks = (key_starts[:, None] + local[None, :]) // SPAN
    allowed = key_blocks[:, :, None] <= (query_positions // SPAN)[None, None, :]
    scores = jnp.where(allowed, scores, -jnp.inf)
    top = jnp.maximum(jnp.max(scores, axis=(0, 1)), -1e30)[None, :]
    expd = jnp.exp(scores - top[None])
    total = jnp.sum(expd, axis=(0, 1))[None, :]
    summed = jnp.einsum(
        "zvk,zkq->vq", blocks[:, NOPE + ROPE :], expd.astype(bf16), preferred_element_type=f32
    )
    packed = jnp.concatenate([summed, top, total, jnp.zeros((6, X * tokens), f32)], axis=0)
    packed = jnp.stack([packed[:, i * tokens : (i + 1) * tokens] for i in range(X)])
    packed, down = lax.optimization_barrier((packed, down))
    packed = exchange(packed, "sp", X_GROUPS)
    tops = packed[:, VDIM]
    factors = jnp.exp(tops - jnp.max(tops, axis=0, keepdims=True))
    merged = jnp.sum(factors[:, None, :] * packed, axis=0)
    attended = (merged[:VDIM] / merged[VDIM + 1 : VDIM + 2]).astype(bf16)
    attended, gate_up_weight, placed = lax.optimization_barrier(
        (attended, gate_up_weight, placed)
    )

    attended_all = lax.all_gather(attended, "tp", axis=0, tiled=True)
    projected = lax.dot_general(
        attended_all, out_weight, (((0,), (0,)), ((), ())), preferred_element_type=f32
    )
    mixed = (residual.astype(f32) + projected).astype(bf16)

    sent = lax.dot_general(placed, mixed, (((0,), (0,)), ((), ())), preferred_element_type=f32)
    arrived = exchange(sent.astype(bf16).reshape(SP, capacity, width), "sp")
    down = down.reshape(Y, 2, ff, width)
    down = jnp.where(core == 0, down, down[:, ::-1]).reshape(Y, 2 * ff, width)
    features = lambda steps: jnp.concatenate([at(down, (y + k) % Y) for k in steps], axis=1)
    down_first, down_above, down_below = features([4]), features([3, 2, 1]), features([-3, -2, -1, 0])
    arrived, down_first, down_above, down_below = lax.optimization_barrier(
        (arrived.reshape(slots, width), down_first, down_above, down_below)
    )

    def products(parts):
        scaled, weights, squares = [], [], 0.0
        for rows, chip, side in parts:
            wide = rows.astype(f32)
            device = (chip % Y) * 2 + side
            scaled.append((wide * at(gains, device)[None, :]).astype(bf16))
            weights.append(at(gate_up_weight, device))
            squares = squares + jnp.sum(wide * wide, axis=1, keepdims=True)
        product = jnp.dot(
            jnp.concatenate(scaled, axis=1),
            jnp.concatenate(weights, axis=0),
            preferred_element_type=f32,
        )
        return product, squares

    half = slots // 2

    def ring(above, below):
        above = y_step(above, 1)
        below = y_step(below, -1)
        return above, below

    above = below = arrived
    gate_up, squares = products([(arrived, y, core), (swap(arrived), y, 1 - core)])
    for k in range(1, 4):
        above, below = ring(above, below)
        crossed = swap(jnp.concatenate([above, below], axis=1))
        more, more_squares = products(
            [
                (above, y - k, core),
                (below, y + k, core),
                (crossed[:, :width], y - k, 1 - core),
                (crossed[:, width:], y + k, 1 - core),
            ]
        )
        gate_up, squares = gate_up + more, squares + more_squares
    last = jnp.concatenate(ring(above[:half], below[half:]), axis=0)
    more, more_squares = products([(last, y + 4, core), (swap(last), y + 4, 1 - core)])
    gate_up, squares = gate_up + more, squares + more_squares
    gate_up = gate_up * lax.rsqrt(squares / D + EPSILON)
    hidden = (jax.nn.silu(gate_up[:, :ff]) * gate_up[:, ff:]).astype(bf16)

    hidden = jnp.concatenate([hidden, swap(hidden)], axis=1)
    first = jnp.dot(hidden, down_first, preferred_element_type=f32).astype(bf16)
    part_above = lax.optimization_barrier(jnp.dot(hidden, down_above, preferred_element_type=f32))
    part_below = lax.optimization_barrier(jnp.dot(hidden, down_below, preferred_element_type=f32))
    column = lambda a, i: a[:, i * width : (i + 1) * width]
    nothing = jnp.zeros((half, width), bf16)
    above = jnp.concatenate([y_step(first[:half], 1), nothing], axis=0)
    below = jnp.concatenate([nothing, y_step(first[half:], -1)], axis=0)
    for i in range(3):
        above = y_step((above.astype(f32) + column(part_above, i)).astype(bf16), 1)
        below = y_step((below.astype(f32) + column(part_below, i)).astype(bf16), -1)
    expert_out = column(part_below, 3) + above.astype(f32) + below.astype(f32)
    expert_out = expert_out.astype(bf16).reshape(SP, capacity, width)

    returned = exchange(expert_out, "sp").reshape(slots, width)
    combine = group_weight[:, None] * route_prob / jnp.sum(route_prob, axis=-1, keepdims=True)
    final = mixed.astype(f32)
    for k in range(TOP):
        picked = jnp.dot(select[k], returned, preferred_element_type=f32)
        final = final + combine[:, k : k + 1] * picked
    return final.astype(bf16)


def solution(mesh):
    return jax.shard_map(
        body,
        mesh=mesh,
        in_specs=(
            P("sp", "tp"),
            P("sp", None),
            P("sp", None),
            P(),
            P(None, "tp"),
            P(None, "tp"),
            P("sp", "tp"),
            P(),
            P("sp", None),
            P("sp", None),
            P("sp"),
            P("sp", None, "tp"),
            P("sp", None, "tp"),
            P("sp", None, "tp"),
        ),
        out_specs=P("sp", "tp"),
        check_vma=False,
    )
```

```python
import jax
import jax.numpy as jnp
from jax import lax
from jax.sharding import PartitionSpec as P

D = 2048
NOPE = 64
ROPE = 32
VDIM = 64
TOP = 2
SPAN = 64
X = 4
Z = 8
Y = 8
SP = X * Z
TP = Y * 2

THETA = 500000.0
EPSILON = 1e-06


Z_GROUPS = [[z * X + x for z in range(Z)] for x in range(X)]
X_GROUPS = [[z * X + x for x in range(X)] for z in range(Z)]


def exchange(value, axis, groups=None):
    return lax.all_to_all(
        value, axis, split_axis=0, concat_axis=0, tiled=True, axis_index_groups=groups
    )


def swap(value):
    return lax.ppermute(value, "tp", [(t, t ^ 1) for t in range(TP)])


def x_shift(value, by):
    return lax.ppermute(
        value, "sp", [(s, s // X * X + (s + by) % X) for s in range(SP)]
    )


def y_step(value, by):
    return lax.ppermute(value, "tp", [(t, (t + 2 * by) % TP) for t in range(TP)])


def tables(positions):
    frequency = 1.0 / THETA ** (jnp.arange(0, ROPE, 2, dtype=jnp.float32) / ROPE)
    angles = positions.astype(jnp.float32)[:, None] * frequency[None, :]
    return jnp.cos(angles), jnp.sin(angles)


def rotate(values, positions):
    half_width = ROPE // 2
    cos_table, sin_table = tables(positions)
    wide = values.astype(jnp.float32)
    lower_half = wide[:, :half_width]
    upper_half = wide[:, half_width:]
    return jnp.concatenate(
        [
            lower_half * cos_table - upper_half * sin_table,
            upper_half * cos_table + lower_half * sin_table,
        ],
        axis=-1,
    ).astype(jnp.bfloat16)


def body(
    queries,
    latent,
    rope_key,
    latent_gain,
    key_value_weight,
    out_weight,
    residual,
    ffn_gain,
    routes,
    route_prob,
    group_weight,
    gate_weight,
    up_weight,
    down_weight,
):
    tokens = queries.shape[0]
    width = residual.shape[1]
    ff = gate_weight.shape[2]
    sp = lax.axis_index("sp")
    tp = lax.axis_index("tp")
    z, x = sp // X, sp % X
    y, core = tp // 2, tp % 2
    bf16, f32 = jnp.bfloat16, jnp.float32
    local = jnp.arange(tokens, dtype=jnp.int32)

    latent_wide = latent.astype(f32)
    normed = latent_wide * lax.rsqrt(
        jnp.mean(latent_wide * latent_wide, axis=-1, keepdims=True) + EPSILON
    )
    normed = (normed * latent_gain.astype(f32)).astype(bf16)
    key_value = lax.dot_general(
        key_value_weight, normed, (((0,), (1,)), ((), ())), preferred_element_type=f32
    ).astype(bf16)
    positions = sp * tokens + local
    rotated = rotate(rope_key, positions).T
    block = jnp.concatenate([key_value[:NOPE], rotated, key_value[NOPE:]], axis=0)
    query = jnp.concatenate([queries[:, :NOPE], rotate(queries[:, NOPE:], positions)], axis=1)
    blocks = exchange(jnp.broadcast_to(block, (Z,) + block.shape), "sp", Z_GROUPS)

    query_parts = [query]
    for by in range(1, X):
        query_parts.append(x_shift(query, by))
    query_parts = jnp.stack(query_parts)
    at = lambda a, chip: lax.dynamic_index_in_dim(a, chip, 0, keepdims=False)
    query_all = jnp.concatenate([at(query_parts, (x - one) % X) for one in range(X)], axis=0)

    gate_up_weight = jnp.concatenate(
        [gate_weight.reshape(TP, width, ff), up_weight.reshape(TP, width, ff)], axis=2
    )
    gains = ffn_gain.astype(f32).reshape(TP, width)
    down = down_weight.reshape(Y // 2, 2, 2 * ff, width)
    odd = y % 2
    parity = lambda one: lax.dynamic_index_in_dim(down, one, 1, keepdims=False)
    kept = parity(odd)
    got = lax.ppermute(parity(1 - odd), "tp", [(t, t ^ 2) for t in range(TP)])
    both = jnp.stack([jnp.where(odd == 0, kept, got), jnp.where(odd == 0, got, kept)], axis=1)
    down = [at(both, y // 2)]
    for by in (1, 2, 3):
        down.append(y_step(at(both, (y // 2 + by) % (Y // 2)), 2 * by))

    experts = SP
    capacity = 2 * tokens * TOP // experts
    slots = experts * capacity
    named = jnp.arange(experts, dtype=jnp.int32)[None, :]
    one_hot = [(routes[:, k : k + 1] == named).astype(f32) for k in range(TOP)]
    both = (one_hot[0] + one_hot[1]).astype(bf16)
    earlier = (local[None, :] < local[:, None]).astype(bf16)
    before = jnp.dot(earlier, both, preferred_element_type=f32)
    slot_row = jnp.arange(slots, dtype=jnp.int32)
    select = []
    for k in range(TOP):
        rank = jnp.sum(before * one_hot[k], axis=1).astype(jnp.int32)
        slot = routes[:, k] * capacity + rank
        select.append((slot[:, None] == slot_row[None, :]).astype(bf16))
    placed = select[0] + select[1]

    scores = jnp.einsum(
        "zdk,qd->zkq", blocks[:, : NOPE + ROPE], query_all, preferred_element_type=f32
    )
    scores = scores * (NOPE + ROPE) ** (-0.5)
    query_positions = z * X * tokens + jnp.arange(X * tokens, dtype=jnp.int32)
    key_starts = (jnp.arange(Z, dtype=jnp.int32) * X + x) * tokens
    key_blocks = (key_starts[:, None] + local[None, :]) // SPAN
    allowed = key_blocks[:, :, None] <= (query_positions // SPAN)[None, None, :]
    scores = jnp.where(allowed, scores, -jnp.inf)
    top = jnp.maximum(jnp.max(scores, axis=(0, 1)), -1e30)[None, :]
    expd = jnp.exp(scores - top[None])
    total = jnp.sum(expd, axis=(0, 1))[None, :]
    summed = jnp.einsum(
        "zvk,zkq->vq", blocks[:, NOPE + ROPE :], expd.astype(bf16), preferred_element_type=f32
    )
    packed = jnp.concatenate([summed, top, total, jnp.zeros((6, X * tokens), f32)], axis=0)
    packed = jnp.stack([packed[:, i * tokens : (i + 1) * tokens] for i in range(X)])
    packed = exchange(packed, "sp", X_GROUPS)
    tops = packed[:, VDIM]
    factors = jnp.exp(tops - jnp.max(tops, axis=0, keepdims=True))
    merged = jnp.sum(factors[:, None, :] * packed, axis=0)
    attended = (merged[:VDIM] / merged[VDIM + 1 : VDIM + 2]).astype(bf16)
    attended, gate_up_weight, placed = lax.optimization_barrier(
        (attended, gate_up_weight, placed)
    )

    attended_all = lax.all_gather(attended, "tp", axis=0, tiled=True)
    projected = lax.dot_general(
        attended_all, out_weight, (((0,), (0,)), ((), ())), preferred_element_type=f32
    )
    mixed = (residual.astype(f32) + projected).astype(bf16)

    sent = lax.dot_general(placed, mixed, (((0,), (0,)), ((), ())), preferred_element_type=f32)
    arrived = exchange(sent.astype(bf16).reshape(SP, capacity, width), "sp")
    down = jnp.stack(down).reshape(Y, 2, ff, width)
    down = jnp.where(core == 0, down, down[:, ::-1]).reshape(Y, 2 * ff, width)

    def features(steps):
        parts = []
        for k in steps:
            chip = (y + k) % Y
            parts.append(at(down, (y // 2 - chip // 2) % (Y // 2) * 2 + chip % 2))
        return jnp.concatenate(parts, axis=1)

    down_first, down_above, down_below = features([4]), features([3, 2, 1]), features([-3, -2, -1, 0])
    arrived, down_first, down_above, down_below = lax.optimization_barrier(
        (arrived.reshape(slots, width), down_first, down_above, down_below)
    )

    def products(parts):
        scaled, weights, squares = [], [], 0.0
        for rows, chip, side in parts:
            wide = rows.astype(f32)
            device = (chip % Y) * 2 + side
            scaled.append((wide * at(gains, device)[None, :]).astype(bf16))
            weights.append(at(gate_up_weight, device))
            squares = squares + jnp.sum(wide * wide, axis=1, keepdims=True)
        product = jnp.dot(
            jnp.concatenate(scaled, axis=1),
            jnp.concatenate(weights, axis=0),
            preferred_element_type=f32,
        )
        return product, squares

    half = slots // 2

    def ring(above, below):
        above = y_step(above, 1)
        below = y_step(below, -1)
        return above, below

    above = below = arrived
    gate_up, squares = products([(arrived, y, core), (swap(arrived), y, 1 - core)])
    for k in range(1, 4):
        above, below = ring(above, below)
        crossed = swap(jnp.concatenate([above, below], axis=1))
        more, more_squares = products(
            [
                (above, y - k, core),
                (below, y + k, core),
                (crossed[:, :width], y - k, 1 - core),
                (crossed[:, width:], y + k, 1 - core),
            ]
        )
        gate_up, squares = gate_up + more, squares + more_squares
    last = jnp.concatenate(ring(above[:half], below[half:]), axis=0)
    more, more_squares = products([(last, y + 4, core), (swap(last), y + 4, 1 - core)])
    gate_up, squares = gate_up + more, squares + more_squares
    gate_up = gate_up * lax.rsqrt(squares / D + EPSILON)
    hidden = (jax.nn.silu(gate_up[:, :ff]) * gate_up[:, ff:]).astype(bf16)

    hidden = jnp.concatenate([hidden, swap(hidden)], axis=1)
    first = jnp.dot(hidden, down_first, preferred_element_type=f32).astype(bf16)
    part_above = lax.optimization_barrier(jnp.dot(hidden, down_above, preferred_element_type=f32))
    part_below = lax.optimization_barrier(jnp.dot(hidden, down_below, preferred_element_type=f32))
    column = lambda a, i: a[:, i * width : (i + 1) * width]
    nothing = jnp.zeros((half, width), bf16)
    above = jnp.concatenate([y_step(first[:half], 1), nothing], axis=0)
    below = jnp.concatenate([nothing, y_step(first[half:], -1)], axis=0)
    for i in range(3):
        above = y_step((above.astype(f32) + column(part_above, i)).astype(bf16), 1)
        below = y_step((below.astype(f32) + column(part_below, i)).astype(bf16), -1)
    expert_out = column(part_below, 3) + above.astype(f32) + below.astype(f32)
    expert_out = expert_out.astype(bf16).reshape(SP, capacity, width)

    returned = exchange(expert_out, "sp").reshape(slots, width)
    combine = group_weight[:, None] * route_prob / jnp.sum(route_prob, axis=-1, keepdims=True)
    final = mixed.astype(f32)
    for k in range(TOP):
        picked = jnp.dot(select[k], returned, preferred_element_type=f32)
        final = final + combine[:, k : k + 1] * picked
    return final.astype(bf16)


def solution(mesh):
    return jax.shard_map(
        body,
        mesh=mesh,
        in_specs=(
            P("sp", "tp"),
            P("sp", None),
            P("sp", None),
            P(),
            P(None, "tp"),
            P(None, "tp"),
            P("sp", "tp"),
            P(),
            P("sp", None),
            P("sp", None),
            P("sp"),
            P("sp", None, "tp"),
            P("sp", None, "tp"),
            P("sp", None, "tp"),
        ),
        out_specs=P("sp", "tp"),
        check_vma=False,
    )
```

```python
import jax
import jax.numpy as jnp
from jax import lax
from jax.sharding import PartitionSpec as P

D = 2048
NOPE = 64
ROPE = 32
VDIM = 64
TOP = 2
SPAN = 64
X = 4
Z = 8
Y = 8
SP = X * Z
TP = Y * 2

THETA = 500000.0
EPSILON = 1e-06


Z_GROUPS = [[z * X + x for z in range(Z)] for x in range(X)]
X_GROUPS = [[z * X + x for x in range(X)] for z in range(Z)]


def exchange(value, axis, groups=None):
    return lax.all_to_all(
        value, axis, split_axis=0, concat_axis=0, tiled=True, axis_index_groups=groups
    )


def swap(value):
    return lax.ppermute(value, "tp", [(t, t ^ 1) for t in range(TP)])


def x_swap(value, bit):
    return lax.ppermute(value, "sp", [(s, s ^ bit) for s in range(SP)])


def y_step(value, by):
    return lax.ppermute(value, "tp", [(t, (t + 2 * by) % TP) for t in range(TP)])


def tables(positions):
    frequency = 1.0 / THETA ** (jnp.arange(0, ROPE, 2, dtype=jnp.float32) / ROPE)
    angles = positions.astype(jnp.float32)[:, None] * frequency[None, :]
    return jnp.cos(angles), jnp.sin(angles)


def rotate(values, positions):
    half_width = ROPE // 2
    cos_table, sin_table = tables(positions)
    wide = values.astype(jnp.float32)
    lower_half = wide[:, :half_width]
    upper_half = wide[:, half_width:]
    return jnp.concatenate(
        [
            lower_half * cos_table - upper_half * sin_table,
            upper_half * cos_table + lower_half * sin_table,
        ],
        axis=-1,
    ).astype(jnp.bfloat16)


def body(
    queries,
    latent,
    rope_key,
    latent_gain,
    key_value_weight,
    out_weight,
    residual,
    ffn_gain,
    routes,
    route_prob,
    group_weight,
    gate_weight,
    up_weight,
    down_weight,
):
    tokens = queries.shape[0]
    width = residual.shape[1]
    ff = gate_weight.shape[2]
    sp = lax.axis_index("sp")
    tp = lax.axis_index("tp")
    z, x = sp // X, sp % X
    y, core = tp // 2, tp % 2
    bf16, f32 = jnp.bfloat16, jnp.float32
    local = jnp.arange(tokens, dtype=jnp.int32)

    latent_wide = latent.astype(f32)
    normed = latent_wide * lax.rsqrt(
        jnp.mean(latent_wide * latent_wide, axis=-1, keepdims=True) + EPSILON
    )
    normed = (normed * latent_gain.astype(f32)).astype(bf16)
    key_value = lax.dot_general(
        key_value_weight, normed, (((0,), (1,)), ((), ())), preferred_element_type=f32
    ).astype(bf16)
    positions = sp * tokens + local
    rotated = rotate(rope_key, positions).T
    block = jnp.concatenate([key_value[:NOPE], rotated, key_value[NOPE:]], axis=0)
    query = jnp.concatenate([queries[:, :NOPE], rotate(queries[:, NOPE:], positions)], axis=1)
    blocks = exchange(jnp.broadcast_to(block, (Z,) + block.shape), "sp", Z_GROUPS)

    query_parts = jnp.stack([query, x_swap(query, 1)])
    query_parts = jnp.concatenate([query_parts, x_swap(query_parts, 2)], axis=0)
    at = lambda a, chip: lax.dynamic_index_in_dim(a, chip, 0, keepdims=False)
    query_all = jnp.concatenate([at(query_parts, x ^ one) for one in range(X)], axis=0)

    down = down_weight.reshape(Y // 2, 2, 2 * ff, width)
    odd = y % 2
    parity = lambda one: lax.dynamic_index_in_dim(down, one, 1, keepdims=False)
    kept = parity(odd)
    got = lax.ppermute(parity(1 - odd), "tp", [(t, t ^ 2) for t in range(TP)])
    both = jnp.stack([jnp.where(odd == 0, kept, got), jnp.where(odd == 0, got, kept)], axis=1)
    down = [at(both, y // 2)]
    for by in (1, 2, 3):
        down.append(y_step(at(both, (y // 2 + by) % (Y // 2)), 2 * by))

    experts = SP
    capacity = 2 * tokens * TOP // experts
    slots = experts * capacity
    named = jnp.arange(experts, dtype=jnp.int32)[None, :]
    one_hot = [(routes[:, k : k + 1] == named).astype(f32) for k in range(TOP)]
    both = (one_hot[0] + one_hot[1]).astype(bf16)
    earlier = (local[None, :] < local[:, None]).astype(bf16)
    before = jnp.dot(earlier, both, preferred_element_type=f32)
    slot_row = jnp.arange(slots, dtype=jnp.int32)
    select = []
    for k in range(TOP):
        rank = jnp.sum(before * one_hot[k], axis=1).astype(jnp.int32)
        slot = routes[:, k] * capacity + rank
        select.append((slot[:, None] == slot_row[None, :]).astype(bf16))
    placed = select[0] + select[1]

    scores = jnp.einsum(
        "zdk,qd->zkq", blocks[:, : NOPE + ROPE], query_all, preferred_element_type=f32
    )
    scores = scores * (NOPE + ROPE) ** (-0.5)
    query_positions = z * X * tokens + jnp.arange(X * tokens, dtype=jnp.int32)
    key_starts = (jnp.arange(Z, dtype=jnp.int32) * X + x) * tokens
    key_blocks = (key_starts[:, None] + local[None, :]) // SPAN
    allowed = key_blocks[:, :, None] <= (query_positions // SPAN)[None, None, :]
    scores = jnp.where(allowed, scores, -jnp.inf)
    top = jnp.maximum(jnp.max(scores, axis=(0, 1)), -1e30)[None, :]
    expd = jnp.exp(scores - top[None])
    total = jnp.sum(expd, axis=(0, 1))[None, :]
    summed = jnp.einsum(
        "zvk,zkq->vq", blocks[:, NOPE + ROPE :], expd.astype(bf16), preferred_element_type=f32
    )
    packed = jnp.concatenate([summed, top, total, jnp.zeros((6, X * tokens), f32)], axis=0)
    packed = jnp.stack([packed[:, i * tokens : (i + 1) * tokens] for i in range(X)])
    packed = exchange(packed, "sp", X_GROUPS)
    tops = packed[:, VDIM]
    factors = jnp.exp(tops - jnp.max(tops, axis=0, keepdims=True))
    merged = jnp.sum(factors[:, None, :] * packed, axis=0)
    attended = (merged[:VDIM] / merged[VDIM + 1 : VDIM + 2]).astype(bf16)
    attended, placed = lax.optimization_barrier((attended, placed))

    attended_all = lax.all_gather(attended, "tp", axis=0, tiled=True)
    projected = lax.dot_general(
        attended_all, out_weight, (((0,), (0,)), ((), ())), preferred_element_type=f32
    )
    mixed = (residual.astype(f32) + projected).astype(bf16)

    sent = lax.dot_general(placed, mixed, (((0,), (0,)), ((), ())), preferred_element_type=f32)
    sent, gate_weight, up_weight, ffn_gain, down = lax.optimization_barrier(
        (sent.astype(bf16), gate_weight, up_weight, ffn_gain, down)
    )
    arrived = exchange(sent.reshape(SP, capacity, width), "sp")
    gate_up_weight = jnp.concatenate(
        [gate_weight.reshape(TP, width, ff), up_weight.reshape(TP, width, ff)], axis=2
    )
    gains = ffn_gain.astype(f32).reshape(TP, width)
    down = jnp.stack(down).reshape(Y, 2, ff, width)
    down = jnp.where(core == 0, down, down[:, ::-1]).reshape(Y, 2 * ff, width)

    def features(steps):
        parts = []
        for k in steps:
            chip = (y + k) % Y
            parts.append(at(down, (y // 2 - chip // 2) % (Y // 2) * 2 + chip % 2))
        return jnp.concatenate(parts, axis=1)

    down_first, down_above, down_below = features([4]), features([3, 2, 1]), features([-3, -2, -1, 0])
    arrived, gate_up_weight, gains, down_first, down_above, down_below = lax.optimization_barrier(
        (arrived.reshape(slots, width), gate_up_weight, gains, down_first, down_above, down_below)
    )

    def products(parts):
        scaled, weights, squares = [], [], 0.0
        for rows, chip, side in parts:
            wide = rows.astype(f32)
            device = (chip % Y) * 2 + side
            scaled.append((wide * at(gains, device)[None, :]).astype(bf16))
            weights.append(at(gate_up_weight, device))
            squares = squares + jnp.sum(wide * wide, axis=1, keepdims=True)
        product = jnp.dot(
            jnp.concatenate(scaled, axis=1),
            jnp.concatenate(weights, axis=0),
            preferred_element_type=f32,
        )
        return product, squares

    half = slots // 2

    def ring(above, below):
        above = y_step(above, 1)
        below = y_step(below, -1)
        return above, below

    above = below = arrived
    gate_up, squares = products([(arrived, y, core), (swap(arrived), y, 1 - core)])
    for k in range(1, 4):
        above, below = ring(above, below)
        crossed = swap(jnp.concatenate([above, below], axis=1))
        more, more_squares = products(
            [
                (above, y - k, core),
                (below, y + k, core),
                (crossed[:, :width], y - k, 1 - core),
                (crossed[:, width:], y + k, 1 - core),
            ]
        )
        gate_up, squares = gate_up + more, squares + more_squares
    last = jnp.concatenate(ring(above[:half], below[half:]), axis=0)
    more, more_squares = products([(last, y + 4, core), (swap(last), y + 4, 1 - core)])
    gate_up, squares = gate_up + more, squares + more_squares
    gate_up = gate_up * lax.rsqrt(squares / D + EPSILON)
    hidden = (jax.nn.silu(gate_up[:, :ff]) * gate_up[:, ff:]).astype(bf16)

    hidden = jnp.concatenate([hidden, swap(hidden)], axis=1)
    first = jnp.dot(hidden, down_first, preferred_element_type=f32).astype(bf16)
    part_above = lax.optimization_barrier(jnp.dot(hidden, down_above, preferred_element_type=f32))
    part_below = lax.optimization_barrier(jnp.dot(hidden, down_below, preferred_element_type=f32))
    column = lambda a, i: a[:, i * width : (i + 1) * width]
    nothing = jnp.zeros((half, width), bf16)
    above = jnp.concatenate([y_step(first[:half], 1), nothing], axis=0)
    below = jnp.concatenate([nothing, y_step(first[half:], -1)], axis=0)
    for i in range(3):
        above = y_step((above.astype(f32) + column(part_above, i)).astype(bf16), 1)
        below = y_step((below.astype(f32) + column(part_below, i)).astype(bf16), -1)
    expert_out = column(part_below, 3) + above.astype(f32) + below.astype(f32)
    expert_out = expert_out.astype(bf16).reshape(SP, capacity, width)

    returned = exchange(expert_out, "sp").reshape(slots, width)
    combine = group_weight[:, None] * route_prob / jnp.sum(route_prob, axis=-1, keepdims=True)
    final = mixed.astype(f32)
    for k in range(TOP):
        picked = jnp.dot(select[k], returned, preferred_element_type=f32)
        final = final + combine[:, k : k + 1] * picked
    return final.astype(bf16)


def solution(mesh):
    return jax.shard_map(
        body,
        mesh=mesh,
        in_specs=(
            P("sp", "tp"),
            P("sp", None),
            P("sp", None),
            P(),
            P(None, "tp"),
            P(None, "tp"),
            P("sp", "tp"),
            P(),
            P("sp", None),
            P("sp", None),
            P("sp"),
            P("sp", None, "tp"),
            P("sp", None, "tp"),
            P("sp", None, "tp"),
        ),
        out_specs=P("sp", "tp"),
        check_vma=False,
    )
```

```python
import jax
import jax.numpy as jnp
from jax import lax
from jax.sharding import PartitionSpec as P

D = 2048
NOPE = 64
ROPE = 32
VDIM = 64
TOP = 2
SPAN = 64
X = 4
Z = 8
Y = 8
SP = X * Z
TP = Y * 2

THETA = 500000.0
EPSILON = 1e-06


Z_GROUPS = [[z * X + x for z in range(Z)] for x in range(X)]
X_GROUPS = [[z * X + x for x in range(X)] for z in range(Z)]


def exchange(value, axis, groups=None):
    return lax.all_to_all(
        value, axis, split_axis=0, concat_axis=0, tiled=True, axis_index_groups=groups
    )


def swap(value):
    return lax.ppermute(value, "tp", [(t, t ^ 1) for t in range(TP)])


def x_swap(value, bit):
    return lax.ppermute(value, "sp", [(s, s ^ bit) for s in range(SP)])


def y_step(value, by):
    return lax.ppermute(value, "tp", [(t, (t + 2 * by) % TP) for t in range(TP)])


def tables(positions):
    frequency = 1.0 / THETA ** (jnp.arange(0, ROPE, 2, dtype=jnp.float32) / ROPE)
    angles = positions.astype(jnp.float32)[:, None] * frequency[None, :]
    return jnp.cos(angles), jnp.sin(angles)


def rotate(values, positions):
    half_width = ROPE // 2
    cos_table, sin_table = tables(positions)
    wide = values.astype(jnp.float32)
    lower_half = wide[:, :half_width]
    upper_half = wide[:, half_width:]
    return jnp.concatenate(
        [
            lower_half * cos_table - upper_half * sin_table,
            upper_half * cos_table + lower_half * sin_table,
        ],
        axis=-1,
    ).astype(jnp.bfloat16)


def body(
    queries,
    latent,
    rope_key,
    latent_gain,
    key_value_weight,
    out_weight,
    residual,
    ffn_gain,
    routes,
    route_prob,
    group_weight,
    gate_weight,
    up_weight,
    down_weight,
):
    tokens = queries.shape[0]
    width = residual.shape[1]
    ff = gate_weight.shape[2]
    sp = lax.axis_index("sp")
    tp = lax.axis_index("tp")
    z, x = sp // X, sp % X
    y, core = tp // 2, tp % 2
    bf16, f32 = jnp.bfloat16, jnp.float32
    local = jnp.arange(tokens, dtype=jnp.int32)

    latent_wide = latent.astype(f32)
    normed = latent_wide * lax.rsqrt(
        jnp.mean(latent_wide * latent_wide, axis=-1, keepdims=True) + EPSILON
    )
    normed = (normed * latent_gain.astype(f32)).astype(bf16)
    key_value = lax.dot_general(
        key_value_weight, normed, (((0,), (1,)), ((), ())), preferred_element_type=f32
    ).astype(bf16)
    positions = sp * tokens + local
    rotated = rotate(rope_key, positions).T
    block = jnp.concatenate([key_value[:NOPE], rotated, key_value[NOPE:]], axis=0)
    query = jnp.concatenate([queries[:, :NOPE], rotate(queries[:, NOPE:], positions)], axis=1)
    blocks = exchange(jnp.broadcast_to(block, (Z,) + block.shape), "sp", Z_GROUPS)

    query_parts = jnp.stack([query, x_swap(query, 1)])
    query_parts = jnp.concatenate([query_parts, x_swap(query_parts, 2)], axis=0)
    at = lambda a, chip: lax.dynamic_index_in_dim(a, chip, 0, keepdims=False)
    query_all = jnp.concatenate([at(query_parts, x ^ one) for one in range(X)], axis=0)

    down = down_weight.reshape(Y // 2, 2, 2 * ff, width)
    odd = y % 2
    parity = lambda one: lax.dynamic_index_in_dim(down, one, 1, keepdims=False)
    kept = parity(odd)
    got = lax.ppermute(parity(1 - odd), "tp", [(t, t ^ 2) for t in range(TP)])
    both = [jnp.where(odd == 0, kept, got), jnp.where(odd == 0, got, kept)]
    both = jnp.concatenate(both, axis=2)
    down = [at(both, y // 2)]
    for by in (1, 2, 3):
        down.append(y_step(at(both, (y // 2 + by) % (Y // 2)), 2 * by))

    experts = SP
    capacity = 2 * tokens * TOP // experts
    slots = experts * capacity
    named = jnp.arange(experts, dtype=jnp.int32)[None, :]
    one_hot = [(routes[:, k : k + 1] == named).astype(f32) for k in range(TOP)]
    both = (one_hot[0] + one_hot[1]).astype(bf16)
    earlier = (local[None, :] < local[:, None]).astype(bf16)
    before = jnp.dot(earlier, both, preferred_element_type=f32)
    slot_row = jnp.arange(slots, dtype=jnp.int32)
    select = []
    for k in range(TOP):
        rank = jnp.sum(before * one_hot[k], axis=1).astype(jnp.int32)
        slot = routes[:, k] * capacity + rank
        select.append((slot[:, None] == slot_row[None, :]).astype(bf16))
    placed = select[0] + select[1]

    scores = jnp.einsum(
        "zdk,qd->zkq", blocks[:, : NOPE + ROPE], query_all, preferred_element_type=f32
    )
    scores = scores * (NOPE + ROPE) ** (-0.5)
    query_positions = z * X * tokens + jnp.arange(X * tokens, dtype=jnp.int32)
    key_starts = (jnp.arange(Z, dtype=jnp.int32) * X + x) * tokens
    key_blocks = (key_starts[:, None] + local[None, :]) // SPAN
    allowed = key_blocks[:, :, None] <= (query_positions // SPAN)[None, None, :]
    scores = jnp.where(allowed, scores, -jnp.inf)
    top = jnp.maximum(jnp.max(scores, axis=(0, 1)), -1e30)[None, :]
    expd = jnp.exp(scores - top[None])
    total = jnp.sum(expd, axis=(0, 1))[None, :]
    summed = jnp.einsum(
        "zvk,zkq->vq", blocks[:, NOPE + ROPE :], expd.astype(bf16), preferred_element_type=f32
    )
    packed = jnp.concatenate([summed, top, total, jnp.zeros((6, X * tokens), f32)], axis=0)
    packed = jnp.stack([packed[:, i * tokens : (i + 1) * tokens] for i in range(X)])
    packed = exchange(packed, "sp", X_GROUPS)
    tops = packed[:, VDIM]
    factors = jnp.exp(tops - jnp.max(tops, axis=0, keepdims=True))
    merged = jnp.sum(factors[:, None, :] * packed, axis=0)
    attended = (merged[:VDIM] / merged[VDIM + 1 : VDIM + 2]).astype(bf16)
    attended, placed = lax.optimization_barrier((attended, placed))

    attended_all = lax.all_gather(attended, "tp", axis=0, tiled=True)
    projected = lax.dot_general(
        attended_all, out_weight, (((0,), (0,)), ((), ())), preferred_element_type=f32
    )
    mixed = (residual.astype(f32) + projected).astype(bf16)

    sent = lax.dot_general(placed, mixed, (((0,), (0,)), ((), ())), preferred_element_type=f32)
    sent, gate_weight, up_weight, ffn_gain = lax.optimization_barrier(
        (sent.astype(bf16), gate_weight, up_weight, ffn_gain)
    )
    arrived = exchange(sent.reshape(SP, capacity, width), "sp")
    gate_up_weight = jnp.concatenate(
        [gate_weight.reshape(TP, width, ff), up_weight.reshape(TP, width, ff)], axis=2
    )
    gains = ffn_gain.astype(f32).reshape(TP, width)
    arrived, gate_up_weight, gains = lax.optimization_barrier(
        (arrived.reshape(slots, width), gate_up_weight, gains)
    )

    def products(parts):
        scaled, weights, squares = [], [], 0.0
        for rows, chip, side in parts:
            wide = rows.astype(f32)
            device = (chip % Y) * 2 + side
            scaled.append((wide * at(gains, device)[None, :]).astype(bf16))
            weights.append(at(gate_up_weight, device))
            squares = squares + jnp.sum(wide * wide, axis=1, keepdims=True)
        product = jnp.dot(
            jnp.concatenate(scaled, axis=1),
            jnp.concatenate(weights, axis=0),
            preferred_element_type=f32,
        )
        return product, squares

    def ring(above, below):
        above = y_step(above, 1)
        below = y_step(below, -1)
        return above, below

    above = below = arrived
    opposite = y_step(arrived, 4)
    gate_up, squares = products([(arrived, y, core), (swap(arrived), y, 1 - core)])
    for k in range(1, 4):
        above, below = ring(above, below)
        blocks = [(above, y - k), (below, y + k)]
        if k == 3:
            above, below, opposite = lax.optimization_barrier((above, below, opposite))
            blocks = [(above, y - k), (below, y + k), (opposite, y + 4)]
        crossed = swap(jnp.concatenate([rows for rows, _ in blocks], axis=1))
        parts = [(rows, chip, core) for rows, chip in blocks]
        for i, (_, chip) in enumerate(blocks):
            parts.append((crossed[:, i * width : (i + 1) * width], chip, 1 - core))
        count = len(blocks)
        for group in ((0, 1, count, count + 1), (2, 5))[: count - 1]:
            more, more_squares = products([parts[i] for i in group])
            gate_up, squares = gate_up + more, squares + more_squares
    gate_up = gate_up * lax.rsqrt(squares / D + EPSILON)
    hidden = (jax.nn.silu(gate_up[:, :ff]) * gate_up[:, ff:]).astype(bf16)

    other = swap(hidden)
    hidden = jnp.where(
        core == 0,
        jnp.concatenate([hidden, other], axis=1),
        jnp.concatenate([other, hidden], axis=1),
    )
    pairs = [
        lax.optimization_barrier(jnp.dot(hidden, one, preferred_element_type=f32)) for one in down
    ]

    def term(by):
        for r in range(Y // 2):
            for h in range(2):
                columns = pairs[r][:, h * width : (h + 1) * width]
                if (h - 2 * r - by) % Y == 0:
                    even_part = columns
                if (h - 2 * r - 1 - by) % Y == 0:
                    odd_part = columns
        return jnp.where(odd == 0, even_part, odd_part)

    above, below = term(3).astype(bf16), term(-3).astype(bf16)
    for k in (2, 1, 0):
        above = y_step(above, 1)
        below = y_step(below, -1)
        if k == 2:
            opposite = y_step(term(4).astype(bf16), 4)
        if k > 0:
            above = (above.astype(f32) + term(k)).astype(bf16)
            below = (below.astype(f32) + term(-k)).astype(bf16)
    expert_out = term(0) + above.astype(f32) + below.astype(f32) + opposite.astype(f32)
    expert_out = expert_out.astype(bf16).reshape(SP, capacity, width)

    returned = exchange(expert_out, "sp").reshape(slots, width)
    combine = group_weight[:, None] * route_prob / jnp.sum(route_prob, axis=-1, keepdims=True)
    final = mixed.astype(f32)
    for k in range(TOP):
        picked = jnp.dot(select[k], returned, preferred_element_type=f32)
        final = final + combine[:, k : k + 1] * picked
    return final.astype(bf16)


def solution(mesh):
    return jax.shard_map(
        body,
        mesh=mesh,
        in_specs=(
            P("sp", "tp"),
            P("sp", None),
            P("sp", None),
            P(),
            P(None, "tp"),
            P(None, "tp"),
            P("sp", "tp"),
            P(),
            P("sp", None),
            P("sp", None),
            P("sp"),
            P("sp", None, "tp"),
            P("sp", None, "tp"),
            P("sp", None, "tp"),
        ),
        out_specs=P("sp", "tp"),
        check_vma=False,
    )
```

```python
import jax
import jax.numpy as jnp
from jax import lax
from jax.sharding import PartitionSpec as P

D = 2048
NOPE = 64
ROPE = 32
VDIM = 64
TOP = 2
SPAN = 64
X = 4
Z = 8
Y = 8
SP = X * Z
TP = Y * 2

THETA = 500000.0
EPSILON = 1e-06


Z_GROUPS = [[z * X + x for z in range(Z)] for x in range(X)]
X_GROUPS = [[z * X + x for x in range(X)] for z in range(Z)]


def exchange(value, axis, groups=None):
    return lax.all_to_all(
        value, axis, split_axis=0, concat_axis=0, tiled=True, axis_index_groups=groups
    )


def swap(value):
    return lax.ppermute(value, "tp", [(t, t ^ 1) for t in range(TP)])


def x_swap(value, bit):
    return lax.ppermute(value, "sp", [(s, s ^ bit) for s in range(SP)])


def y_step(value, by):
    return lax.ppermute(value, "tp", [(t, (t + 2 * by) % TP) for t in range(TP)])


def tables(positions):
    frequency = 1.0 / THETA ** (jnp.arange(0, ROPE, 2, dtype=jnp.float32) / ROPE)
    angles = positions.astype(jnp.float32)[:, None] * frequency[None, :]
    return jnp.cos(angles), jnp.sin(angles)


def rotate(values, positions):
    half_width = ROPE // 2
    cos_table, sin_table = tables(positions)
    wide = values.astype(jnp.float32)
    lower_half = wide[:, :half_width]
    upper_half = wide[:, half_width:]
    return jnp.concatenate(
        [
            lower_half * cos_table - upper_half * sin_table,
            upper_half * cos_table + lower_half * sin_table,
        ],
        axis=-1,
    ).astype(jnp.bfloat16)


def body(
    queries,
    latent,
    rope_key,
    latent_gain,
    key_value_weight,
    out_weight,
    residual,
    ffn_gain,
    routes,
    route_prob,
    group_weight,
    gate_weight,
    up_weight,
    down_weight,
):
    tokens = queries.shape[0]
    width = residual.shape[1]
    ff = gate_weight.shape[2]
    sp = lax.axis_index("sp")
    tp = lax.axis_index("tp")
    z, x = sp // X, sp % X
    y, core = tp // 2, tp % 2
    bf16, f32 = jnp.bfloat16, jnp.float32
    local = jnp.arange(tokens, dtype=jnp.int32)

    latent_wide = latent.astype(f32)
    normed = latent_wide * lax.rsqrt(
        jnp.mean(latent_wide * latent_wide, axis=-1, keepdims=True) + EPSILON
    )
    normed = (normed * latent_gain.astype(f32)).astype(bf16)
    key_value = lax.dot_general(
        key_value_weight, normed, (((0,), (1,)), ((), ())), preferred_element_type=f32
    ).astype(bf16)
    positions = sp * tokens + local
    rotated = rotate(rope_key, positions).T
    block = jnp.concatenate([key_value[:NOPE], rotated, key_value[NOPE:]], axis=0)
    block, queries = lax.optimization_barrier((block, queries))
    query = jnp.concatenate([queries[:, :NOPE], rotate(queries[:, NOPE:], positions)], axis=1)
    blocks = exchange(jnp.broadcast_to(block, (Z,) + block.shape), "sp", Z_GROUPS)

    query_parts = jnp.stack([query, x_swap(query, 1)])
    query_parts = jnp.concatenate([query_parts, x_swap(query_parts, 2)], axis=0)
    at = lambda a, chip: lax.dynamic_index_in_dim(a, chip, 0, keepdims=False)
    query_all = jnp.concatenate([at(query_parts, x ^ one) for one in range(X)], axis=0)

    down = down_weight.reshape(Y // 2, 2, 2 * ff, width)
    odd = y % 2
    parity = lambda one: lax.dynamic_index_in_dim(down, one, 1, keepdims=False)
    kept = parity(odd)
    got = lax.ppermute(parity(1 - odd), "tp", [(t, t ^ 2) for t in range(TP)])
    both = [jnp.where(odd == 0, kept, got), jnp.where(odd == 0, got, kept)]
    both = jnp.concatenate(both, axis=2)
    down = [at(both, y // 2)]
    for by in (1, 2, 3):
        down.append(y_step(at(both, (y // 2 + by) % (Y // 2)), 2 * by))

    experts = SP
    capacity = 2 * tokens * TOP // experts
    slots = experts * capacity
    named = jnp.arange(experts, dtype=jnp.int32)[None, :]
    one_hot = [(routes[:, k : k + 1] == named).astype(f32) for k in range(TOP)]
    both = (one_hot[0] + one_hot[1]).astype(bf16)
    earlier = (local[None, :] < local[:, None]).astype(bf16)
    before = jnp.dot(earlier, both, preferred_element_type=f32)
    slot_row = jnp.arange(slots, dtype=jnp.int32)
    select = []
    for k in range(TOP):
        rank = jnp.sum(before * one_hot[k], axis=1).astype(jnp.int32)
        slot = routes[:, k] * capacity + rank
        select.append((slot[:, None] == slot_row[None, :]).astype(bf16))
    placed = select[0] + select[1]

    scores = jnp.einsum(
        "zdk,qd->zkq", blocks[:, : NOPE + ROPE], query_all, preferred_element_type=f32
    )
    scores = scores * (NOPE + ROPE) ** (-0.5)
    query_positions = z * X * tokens + jnp.arange(X * tokens, dtype=jnp.int32)
    key_starts = (jnp.arange(Z, dtype=jnp.int32) * X + x) * tokens
    key_blocks = (key_starts[:, None] + local[None, :]) // SPAN
    allowed = key_blocks[:, :, None] <= (query_positions // SPAN)[None, None, :]
    scores = jnp.where(allowed, scores, -jnp.inf)
    top = jnp.maximum(jnp.max(scores, axis=(0, 1)), -1e30)[None, :]
    expd = jnp.exp(scores - top[None])
    total = jnp.sum(expd, axis=(0, 1))[None, :]
    summed = jnp.einsum(
        "zvk,zkq->vq", blocks[:, NOPE + ROPE :], expd.astype(bf16), preferred_element_type=f32
    )
    packed = jnp.concatenate([summed, top, total, jnp.zeros((6, X * tokens), f32)], axis=0)
    packed = jnp.stack([packed[:, i * tokens : (i + 1) * tokens] for i in range(X)])
    packed = exchange(packed, "sp", X_GROUPS)
    tops = packed[:, VDIM]
    factors = jnp.exp(tops - jnp.max(tops, axis=0, keepdims=True))
    merged = jnp.sum(factors[:, None, :] * packed, axis=0)
    attended = (merged[:VDIM] / merged[VDIM + 1 : VDIM + 2]).astype(bf16)
    attended, placed = lax.optimization_barrier((attended, placed))

    attended_all = lax.all_gather(attended, "tp", axis=0, tiled=True)
    projected = lax.dot_general(
        attended_all, out_weight, (((0,), (0,)), ((), ())), preferred_element_type=f32
    )
    mixed = (residual.astype(f32) + projected).astype(bf16)

    sent = lax.dot_general(placed, mixed, (((0,), (0,)), ((), ())), preferred_element_type=f32)
    sent, gate_weight, up_weight, ffn_gain = lax.optimization_barrier(
        (sent.astype(bf16), gate_weight, up_weight, ffn_gain)
    )
    arrived = exchange(sent.reshape(SP, capacity, width), "sp")
    gate_up_weight = jnp.concatenate(
        [gate_weight.reshape(TP, width, ff), up_weight.reshape(TP, width, ff)], axis=2
    )
    gains = ffn_gain.astype(f32).reshape(TP, width)
    arrived, gate_up_weight, gains = lax.optimization_barrier(
        (arrived.reshape(slots, width), gate_up_weight, gains)
    )

    def products(parts):
        scaled, weights, squares = [], [], 0.0
        for rows, chip, side in parts:
            wide = rows.astype(f32)
            device = (chip % Y) * 2 + side
            scaled.append((wide * at(gains, device)[None, :]).astype(bf16))
            weights.append(at(gate_up_weight, device))
            squares = squares + jnp.sum(wide * wide, axis=1, keepdims=True)
        product = jnp.dot(
            jnp.concatenate(scaled, axis=1),
            jnp.concatenate(weights, axis=0),
            preferred_element_type=f32,
        )
        return product, squares

    def ring(above, below):
        above = y_step(above, 1)
        below = y_step(below, -1)
        return above, below

    half = slots // 2
    above = below = arrived
    gate_up, squares = products([(arrived, y, core), (swap(arrived), y, 1 - core)])
    for k in range(1, 4):
        above, below = ring(above, below)
        crossed = swap(jnp.concatenate([above, below], axis=1))
        more, more_squares = products(
            [
                (above, y - k, core),
                (below, y + k, core),
                (crossed[:, :width], y - k, 1 - core),
                (crossed[:, width:], y + k, 1 - core),
            ]
        )
        gate_up, squares = gate_up + more, squares + more_squares
    last = jnp.concatenate(ring(above[:half], below[half:]), axis=0)
    last, down = lax.optimization_barrier((last, down))

    def features(steps):
        parts = []
        for by in steps:
            for r in range(Y // 2):
                for h in range(2):
                    columns = down[r][:, h * width : (h + 1) * width]
                    if (h - 2 * r - by) % Y == 0:
                        even_part = columns
                    if (h - 2 * r - 1 - by) % Y == 0:
                        odd_part = columns
            parts.append(jnp.where(odd == 0, even_part, odd_part))
        return jnp.concatenate(parts, axis=1)

    down_first, down_above, down_below = features([4]), features([3, 2, 1]), features([-3, -2, -1, 0])
    more, more_squares = products([(last, y + 4, core), (swap(last), y + 4, 1 - core)])
    gate_up, squares = gate_up + more, squares + more_squares
    gate_up = gate_up * lax.rsqrt(squares / D + EPSILON)
    hidden = (jax.nn.silu(gate_up[:, :ff]) * gate_up[:, ff:]).astype(bf16)

    other = swap(hidden)
    hidden = jnp.where(
        core == 0,
        jnp.concatenate([hidden, other], axis=1),
        jnp.concatenate([other, hidden], axis=1),
    )
    hidden = lax.optimization_barrier(hidden)
    first = jnp.dot(hidden, down_first, preferred_element_type=f32).astype(bf16)
    part_above = lax.optimization_barrier(jnp.dot(hidden, down_above, preferred_element_type=f32))
    part_below = lax.optimization_barrier(jnp.dot(hidden, down_below, preferred_element_type=f32))
    column = lambda a, i: a[:, i * width : (i + 1) * width]
    nothing = jnp.zeros((half, width), bf16)
    above = jnp.concatenate([y_step(first[:half], 1), nothing], axis=0)
    below = jnp.concatenate([nothing, y_step(first[half:], -1)], axis=0)
    for i in range(3):
        above = y_step((above.astype(f32) + column(part_above, i)).astype(bf16), 1)
        below = y_step((below.astype(f32) + column(part_below, i)).astype(bf16), -1)
    expert_out = column(part_below, 3) + above.astype(f32) + below.astype(f32)
    expert_out = expert_out.astype(bf16).reshape(SP, capacity, width)

    returned = exchange(expert_out, "sp").reshape(slots, width)
    combine = group_weight[:, None] * route_prob / jnp.sum(route_prob, axis=-1, keepdims=True)
    final = mixed.astype(f32)
    for k in range(TOP):
        picked = jnp.dot(select[k], returned, preferred_element_type=f32)
        final = final + combine[:, k : k + 1] * picked
    return final.astype(bf16)


def solution(mesh):
    return jax.shard_map(
        body,
        mesh=mesh,
        in_specs=(
            P("sp", "tp"),
            P("sp", None),
            P("sp", None),
            P(),
            P(None, "tp"),
            P(None, "tp"),
            P("sp", "tp"),
            P(),
            P("sp", None),
            P("sp", None),
            P("sp"),
            P("sp", None, "tp"),
            P("sp", None, "tp"),
            P("sp", None, "tp"),
        ),
        out_specs=P("sp", "tp"),
        check_vma=False,
    )
```

```python
import jax
import jax.numpy as jnp
from jax import lax
from jax.sharding import PartitionSpec as P

D = 2048
NOPE = 64
ROPE = 32
VDIM = 64
TOP = 2
SPAN = 64
X = 4
Z = 8
Y = 8
SP = X * Z
TP = Y * 2

THETA = 500000.0
EPSILON = 1e-06


Z_GROUPS = [[z * X + x for z in range(Z)] for x in range(X)]
X_GROUPS = [[z * X + x for x in range(X)] for z in range(Z)]


def exchange(value, axis, groups=None):
    return lax.all_to_all(
        value, axis, split_axis=0, concat_axis=0, tiled=True, axis_index_groups=groups
    )


def swap(value):
    return lax.ppermute(value, "tp", [(t, t ^ 1) for t in range(TP)])


def x_swap(value, bit):
    return lax.ppermute(value, "sp", [(s, s ^ bit) for s in range(SP)])


def y_step(value, by):
    return lax.ppermute(value, "tp", [(t, (t + 2 * by) % TP) for t in range(TP)])


def tables(positions):
    frequency = 1.0 / THETA ** (jnp.arange(0, ROPE, 2, dtype=jnp.float32) / ROPE)
    angles = positions.astype(jnp.float32)[:, None] * frequency[None, :]
    return jnp.cos(angles), jnp.sin(angles)


def rotate(values, positions):
    half_width = ROPE // 2
    cos_table, sin_table = tables(positions)
    wide = values.astype(jnp.float32)
    lower_half = wide[:, :half_width]
    upper_half = wide[:, half_width:]
    return jnp.concatenate(
        [
            lower_half * cos_table - upper_half * sin_table,
            upper_half * cos_table + lower_half * sin_table,
        ],
        axis=-1,
    ).astype(jnp.bfloat16)


def body(
    queries,
    latent,
    rope_key,
    latent_gain,
    key_value_weight,
    out_weight,
    residual,
    ffn_gain,
    routes,
    route_prob,
    group_weight,
    gate_weight,
    up_weight,
    down_weight,
):
    tokens = queries.shape[0]
    width = residual.shape[1]
    ff = gate_weight.shape[2]
    sp = lax.axis_index("sp")
    tp = lax.axis_index("tp")
    z, x = sp // X, sp % X
    y, core = tp // 2, tp % 2
    bf16, f32 = jnp.bfloat16, jnp.float32
    local = jnp.arange(tokens, dtype=jnp.int32)

    latent_wide = latent.astype(f32)
    normed = latent_wide * lax.rsqrt(
        jnp.mean(latent_wide * latent_wide, axis=-1, keepdims=True) + EPSILON
    )
    normed = (normed * latent_gain.astype(f32)).astype(bf16)
    key_value = lax.dot_general(
        key_value_weight, normed, (((0,), (1,)), ((), ())), preferred_element_type=f32
    ).astype(bf16)
    positions = sp * tokens + local
    rotated = rotate(rope_key, positions).T
    block = jnp.concatenate([key_value[:NOPE], rotated, key_value[NOPE:]], axis=0)
    block, queries = lax.optimization_barrier((block, queries))
    query = jnp.concatenate([queries[:, :NOPE], rotate(queries[:, NOPE:], positions)], axis=1)
    blocks = exchange(jnp.broadcast_to(block, (Z,) + block.shape), "sp", Z_GROUPS)

    query_parts = jnp.stack([query, x_swap(query, 1)])
    query_parts = jnp.concatenate([query_parts, x_swap(query_parts, 2)], axis=0)
    at = lambda a, chip: lax.dynamic_index_in_dim(a, chip, 0, keepdims=False)
    query_all = jnp.concatenate([at(query_parts, x ^ one) for one in range(X)], axis=0)

    down = down_weight.reshape(Y // 2, 2, 2 * ff, width)
    odd = y % 2
    parity = lambda one: lax.dynamic_index_in_dim(down, one, 1, keepdims=False)
    kept = parity(odd)
    got = lax.ppermute(parity(1 - odd), "tp", [(t, t ^ 2) for t in range(TP)])
    both = [jnp.where(odd == 0, kept, got), jnp.where(odd == 0, got, kept)]
    both = jnp.concatenate(both, axis=2)
    down = [at(both, y // 2)]
    for by in (1, 2, 3):
        down.append(y_step(at(both, (y // 2 + by) % (Y // 2)), 2 * by))

    experts = SP
    capacity = 2 * tokens * TOP // experts
    slots = experts * capacity
    named = jnp.arange(experts, dtype=jnp.int32)[None, :]
    one_hot = [(routes[:, k : k + 1] == named).astype(f32) for k in range(TOP)]
    both = (one_hot[0] + one_hot[1]).astype(bf16)
    earlier = (local[None, :] < local[:, None]).astype(bf16)
    before = jnp.dot(earlier, both, preferred_element_type=f32)
    slot_row = jnp.arange(slots, dtype=jnp.int32)
    select = []
    for k in range(TOP):
        rank = jnp.sum(before * one_hot[k], axis=1).astype(jnp.int32)
        slot = routes[:, k] * capacity + rank
        select.append((slot[:, None] == slot_row[None, :]).astype(bf16))
    placed = select[0] + select[1]

    scores = jnp.einsum(
        "zdk,qd->zkq", blocks[:, : NOPE + ROPE], query_all, preferred_element_type=f32
    )
    scores = scores * (NOPE + ROPE) ** (-0.5)
    query_positions = z * X * tokens + jnp.arange(X * tokens, dtype=jnp.int32)
    key_starts = (jnp.arange(Z, dtype=jnp.int32) * X + x) * tokens
    key_blocks = (key_starts[:, None] + local[None, :]) // SPAN
    allowed = key_blocks[:, :, None] <= (query_positions // SPAN)[None, None, :]
    scores = jnp.where(allowed, scores, -jnp.inf)
    top = jnp.maximum(jnp.max(scores, axis=(0, 1)), -1e30)[None, :]
    expd = jnp.exp(scores - top[None])
    total = jnp.sum(expd, axis=(0, 1))[None, :]
    summed = jnp.einsum(
        "zvk,zkq->vq", blocks[:, NOPE + ROPE :], expd.astype(bf16), preferred_element_type=f32
    )
    packed = jnp.concatenate([summed, top, total, jnp.zeros((6, X * tokens), f32)], axis=0)
    packed = jnp.stack([packed[:, i * tokens : (i + 1) * tokens] for i in range(X)])
    packed = exchange(packed, "sp", X_GROUPS)
    tops = packed[:, VDIM]
    factors = jnp.exp(tops - jnp.max(tops, axis=0, keepdims=True))
    merged = jnp.sum(factors[:, None, :] * packed, axis=0)
    attended = (merged[:VDIM] / merged[VDIM + 1 : VDIM + 2]).astype(bf16)
    attended, placed = lax.optimization_barrier((attended, placed))

    attended_all = lax.all_gather(attended, "tp", axis=0, tiled=True)
    projected = lax.dot_general(
        attended_all, out_weight, (((0,), (0,)), ((), ())), preferred_element_type=f32
    )
    mixed = (residual.astype(f32) + projected).astype(bf16)

    sent = lax.dot_general(placed, mixed, (((0,), (0,)), ((), ())), preferred_element_type=f32)
    sent, gate_weight, up_weight, ffn_gain, down = lax.optimization_barrier(
        (sent.astype(bf16), gate_weight, up_weight, ffn_gain, down)
    )
    arrived = exchange(sent.reshape(SP, capacity, width), "sp")
    gate_up_weight = jnp.concatenate(
        [gate_weight.reshape(TP, width, ff), up_weight.reshape(TP, width, ff)], axis=2
    )
    gains = ffn_gain.astype(f32).reshape(TP, width)

    def features(steps):
        parts = []
        for by in steps:
            for r in range(Y // 2):
                for h in range(2):
                    columns = down[r][:, h * width : (h + 1) * width]
                    if (h - 2 * r - by) % Y == 0:
                        even_part = columns
                    if (h - 2 * r - 1 - by) % Y == 0:
                        odd_part = columns
            parts.append(jnp.where(odd == 0, even_part, odd_part))
        return jnp.concatenate(parts, axis=1)

    down_first, down_above, down_below = features([4]), features([3, 2, 1]), features([-3, -2, -1, 0])
    arrived, gate_up_weight, gains, down_first, down_above, down_below = lax.optimization_barrier(
        (arrived.reshape(slots, width), gate_up_weight, gains, down_first, down_above, down_below)
    )

    def products(parts):
        scaled, weights, squares = [], [], 0.0
        for rows, chip, side in parts:
            wide = rows.astype(f32)
            device = (chip % Y) * 2 + side
            scaled.append((wide * at(gains, device)[None, :]).astype(bf16))
            weights.append(at(gate_up_weight, device))
            squares = squares + jnp.sum(wide * wide, axis=1, keepdims=True)
        product = jnp.dot(
            jnp.concatenate(scaled, axis=1),
            jnp.concatenate(weights, axis=0),
            preferred_element_type=f32,
        )
        return product, squares

    def ring(above, below):
        above = y_step(above, 1)
        below = y_step(below, -1)
        return above, below

    half = slots // 2
    above = below = arrived
    gate_up, squares = products([(arrived, y, core), (swap(arrived), y, 1 - core)])
    for k in range(1, 4):
        above, below = ring(above, below)
        crossed = swap(jnp.concatenate([above, below], axis=1))
        more, more_squares = products(
            [
                (above, y - k, core),
                (below, y + k, core),
                (crossed[:, :width], y - k, 1 - core),
                (crossed[:, width:], y + k, 1 - core),
            ]
        )
        gate_up, squares = gate_up + more, squares + more_squares
    last = jnp.concatenate(ring(above[:half], below[half:]), axis=0)
    more, more_squares = products([(last, y + 4, core), (swap(last), y + 4, 1 - core)])
    gate_up, squares = gate_up + more, squares + more_squares
    gate_up = gate_up * lax.rsqrt(squares / D + EPSILON)
    hidden = (jax.nn.silu(gate_up[:, :ff]) * gate_up[:, ff:]).astype(bf16)

    other = swap(hidden)
    hidden = jnp.where(
        core == 0,
        jnp.concatenate([hidden, other], axis=1),
        jnp.concatenate([other, hidden], axis=1),
    )
    hidden = lax.optimization_barrier(hidden)
    first = jnp.dot(hidden, down_first, preferred_element_type=f32).astype(bf16)
    part_above = lax.optimization_barrier(jnp.dot(hidden, down_above, preferred_element_type=f32))
    part_below = lax.optimization_barrier(jnp.dot(hidden, down_below, preferred_element_type=f32))
    column = lambda a, i: a[:, i * width : (i + 1) * width]
    nothing = jnp.zeros((half, width), bf16)
    above = jnp.concatenate([y_step(first[:half], 1), nothing], axis=0)
    below = jnp.concatenate([nothing, y_step(first[half:], -1)], axis=0)
    for i in range(3):
        above = y_step((above.astype(f32) + column(part_above, i)).astype(bf16), 1)
        below = y_step((below.astype(f32) + column(part_below, i)).astype(bf16), -1)
    expert_out = column(part_below, 3) + above.astype(f32) + below.astype(f32)
    expert_out = expert_out.astype(bf16).reshape(SP, capacity, width)

    returned = exchange(expert_out, "sp").reshape(slots, width)
    combine = group_weight[:, None] * route_prob / jnp.sum(route_prob, axis=-1, keepdims=True)
    final = mixed.astype(f32)
    for k in range(TOP):
        picked = jnp.dot(select[k], returned, preferred_element_type=f32)
        final = final + combine[:, k : k + 1] * picked
    return final.astype(bf16)


def solution(mesh):
    return jax.shard_map(
        body,
        mesh=mesh,
        in_specs=(
            P("sp", "tp"),
            P("sp", None),
            P("sp", None),
            P(),
            P(None, "tp"),
            P(None, "tp"),
            P("sp", "tp"),
            P(),
            P("sp", None),
            P("sp", None),
            P("sp"),
            P("sp", None, "tp"),
            P("sp", None, "tp"),
            P("sp", None, "tp"),
        ),
        out_specs=P("sp", "tp"),
        check_vma=False,
    )
```

```python
import jax
import jax.numpy as jnp
from jax import lax
from jax.sharding import PartitionSpec as P

D = 2048
NOPE = 64
ROPE = 32
VDIM = 64
TOP = 2
SPAN = 64
X = 4
Z = 8
Y = 8
SP = X * Z
TP = Y * 2

THETA = 500000.0
EPSILON = 1e-06


Z_GROUPS = [[z * X + x for z in range(Z)] for x in range(X)]
X_GROUPS = [[z * X + x for x in range(X)] for z in range(Z)]


def exchange(value, axis, groups=None):
    return lax.all_to_all(
        value, axis, split_axis=0, concat_axis=0, tiled=True, axis_index_groups=groups
    )


def swap(value):
    return lax.ppermute(value, "tp", [(t, t ^ 1) for t in range(TP)])


def x_swap(value, bit):
    return lax.ppermute(value, "sp", [(s, s ^ bit) for s in range(SP)])


def y_step(value, by):
    return lax.ppermute(value, "tp", [(t, (t + 2 * by) % TP) for t in range(TP)])


def tables(positions):
    frequency = 1.0 / THETA ** (jnp.arange(0, ROPE, 2, dtype=jnp.float32) / ROPE)
    angles = positions.astype(jnp.float32)[:, None] * frequency[None, :]
    return jnp.cos(angles), jnp.sin(angles)


def rotate(values, positions):
    half_width = ROPE // 2
    cos_table, sin_table = tables(positions)
    wide = values.astype(jnp.float32)
    lower_half = wide[:, :half_width]
    upper_half = wide[:, half_width:]
    return jnp.concatenate(
        [
            lower_half * cos_table - upper_half * sin_table,
            upper_half * cos_table + lower_half * sin_table,
        ],
        axis=-1,
    ).astype(jnp.bfloat16)


def body(
    queries,
    latent,
    rope_key,
    latent_gain,
    key_value_weight,
    out_weight,
    residual,
    ffn_gain,
    routes,
    route_prob,
    group_weight,
    gate_weight,
    up_weight,
    down_weight,
):
    tokens = queries.shape[0]
    width = residual.shape[1]
    ff = gate_weight.shape[2]
    sp = lax.axis_index("sp")
    tp = lax.axis_index("tp")
    z, x = sp // X, sp % X
    y, core = tp // 2, tp % 2
    bf16, f32 = jnp.bfloat16, jnp.float32
    local = jnp.arange(tokens, dtype=jnp.int32)

    latent_wide = latent.astype(f32)
    normed = latent_wide * lax.rsqrt(
        jnp.mean(latent_wide * latent_wide, axis=-1, keepdims=True) + EPSILON
    )
    normed = (normed * latent_gain.astype(f32)).astype(bf16)
    key_value = lax.dot_general(
        key_value_weight, normed, (((0,), (1,)), ((), ())), preferred_element_type=f32
    ).astype(bf16)
    positions = sp * tokens + local
    rotated = rotate(rope_key, positions).T
    block = jnp.concatenate([key_value[:NOPE], rotated, key_value[NOPE:]], axis=0)
    block, queries = lax.optimization_barrier((block, queries))
    query = jnp.concatenate([queries[:, :NOPE], rotate(queries[:, NOPE:], positions)], axis=1)
    blocks = exchange(jnp.broadcast_to(block, (Z,) + block.shape), "sp", Z_GROUPS)

    query_parts = jnp.stack([query, x_swap(query, 1)])
    query_parts = jnp.concatenate([query_parts, x_swap(query_parts, 2)], axis=0)
    at = lambda a, chip: lax.dynamic_index_in_dim(a, chip, 0, keepdims=False)
    query_all = jnp.concatenate([at(query_parts, x ^ one) for one in range(X)], axis=0)

    down = down_weight.reshape(Y // 2, 2, 2 * ff, width)
    odd = y % 2
    parts = [at(down, y // 2)]
    for by in (1, 2, 3):
        parts.append(y_step(at(down, (y // 2 + by) % (Y // 2)), 2 * by))
    kept = [at(part, odd) for part in parts]
    given = jnp.stack([at(part, 1 - odd) for part in parts])
    got = lax.ppermute(given, "tp", [(t, t ^ 2) for t in range(TP)])

    experts = SP
    capacity = 2 * tokens * TOP // experts
    slots = experts * capacity
    named = jnp.arange(experts, dtype=jnp.int32)[None, :]
    one_hot = [(routes[:, k : k + 1] == named).astype(f32) for k in range(TOP)]
    both = (one_hot[0] + one_hot[1]).astype(bf16)
    earlier = (local[None, :] < local[:, None]).astype(bf16)
    before = jnp.dot(earlier, both, preferred_element_type=f32)
    slot_row = jnp.arange(slots, dtype=jnp.int32)
    select = []
    for k in range(TOP):
        rank = jnp.sum(before * one_hot[k], axis=1).astype(jnp.int32)
        slot = routes[:, k] * capacity + rank
        select.append((slot[:, None] == slot_row[None, :]).astype(bf16))
    placed = select[0] + select[1]

    scores = jnp.einsum(
        "zdk,qd->zkq", blocks[:, : NOPE + ROPE], query_all, preferred_element_type=f32
    )
    scores = scores * (NOPE + ROPE) ** (-0.5)
    query_positions = z * X * tokens + jnp.arange(X * tokens, dtype=jnp.int32)
    key_starts = (jnp.arange(Z, dtype=jnp.int32) * X + x) * tokens
    key_blocks = (key_starts[:, None] + local[None, :]) // SPAN
    allowed = key_blocks[:, :, None] <= (query_positions // SPAN)[None, None, :]
    scores = jnp.where(allowed, scores, -jnp.inf)
    top = jnp.maximum(jnp.max(scores, axis=(0, 1)), -1e30)[None, :]
    expd = jnp.exp(scores - top[None])
    total = jnp.sum(expd, axis=(0, 1))[None, :]
    summed = jnp.einsum(
        "zvk,zkq->vq", blocks[:, NOPE + ROPE :], expd.astype(bf16), preferred_element_type=f32
    )
    packed = jnp.concatenate([summed, top, total, jnp.zeros((6, X * tokens), f32)], axis=0)
    packed = jnp.stack([packed[:, i * tokens : (i + 1) * tokens] for i in range(X)])
    packed = exchange(packed, "sp", X_GROUPS)
    tops = packed[:, VDIM]
    factors = jnp.exp(tops - jnp.max(tops, axis=0, keepdims=True))
    merged = jnp.sum(factors[:, None, :] * packed, axis=0)
    attended = (merged[:VDIM] / merged[VDIM + 1 : VDIM + 2]).astype(bf16)
    attended, placed = lax.optimization_barrier((attended, placed))

    attended_all = lax.all_gather(attended, "tp", axis=0, tiled=True)
    projected = lax.dot_general(
        attended_all, out_weight, (((0,), (0,)), ((), ())), preferred_element_type=f32
    )
    mixed = (residual.astype(f32) + projected).astype(bf16)

    sent = lax.dot_general(placed, mixed, (((0,), (0,)), ((), ())), preferred_element_type=f32)
    sent, gate_weight, up_weight, ffn_gain, kept, got = lax.optimization_barrier(
        (sent.astype(bf16), gate_weight, up_weight, ffn_gain, kept, got)
    )
    arrived = exchange(sent.reshape(SP, capacity, width), "sp")
    gate_up_weight = jnp.concatenate(
        [gate_weight.reshape(TP, width, ff), up_weight.reshape(TP, width, ff)], axis=2
    )
    gains = ffn_gain.astype(f32).reshape(TP, width)

    def features(steps):
        parts = []
        for by in steps:
            if by % 2 == 0:
                parts.append(kept[-by // 2 % (Y // 2)])
            else:
                even_part = got[(1 - by) // 2 % (Y // 2)]
                odd_part = got[(-1 - by) // 2 % (Y // 2)]
                parts.append(jnp.where(odd == 0, even_part, odd_part))
        return jnp.concatenate(parts, axis=1)

    down_first, down_above, down_below = features([4]), features([3, 2, 1]), features([-3, -2, -1, 0])
    arrived, gate_up_weight, gains, down_first, down_above, down_below = lax.optimization_barrier(
        (arrived.reshape(slots, width), gate_up_weight, gains, down_first, down_above, down_below)
    )

    def products(parts):
        scaled, weights, squares = [], [], 0.0
        for rows, chip, side in parts:
            wide = rows.astype(f32)
            device = (chip % Y) * 2 + side
            scaled.append((wide * at(gains, device)[None, :]).astype(bf16))
            weights.append(at(gate_up_weight, device))
            squares = squares + jnp.sum(wide * wide, axis=1, keepdims=True)
        product = jnp.dot(
            jnp.concatenate(scaled, axis=1),
            jnp.concatenate(weights, axis=0),
            preferred_element_type=f32,
        )
        return product, squares

    def ring(above, below):
        above = y_step(above, 1)
        below = y_step(below, -1)
        return above, below

    half = slots // 2
    above = below = arrived
    gate_up, squares = products([(arrived, y, core), (swap(arrived), y, 1 - core)])
    for k in range(1, 4):
        above, below = ring(above, below)
        crossed = swap(jnp.concatenate([above, below], axis=1))
        more, more_squares = products(
            [
                (above, y - k, core),
                (below, y + k, core),
                (crossed[:, :width], y - k, 1 - core),
                (crossed[:, width:], y + k, 1 - core),
            ]
        )
        gate_up, squares = gate_up + more, squares + more_squares
    last = jnp.concatenate(ring(above[:half], below[half:]), axis=0)
    more, more_squares = products([(last, y + 4, core), (swap(last), y + 4, 1 - core)])
    gate_up, squares = gate_up + more, squares + more_squares
    gate_up = gate_up * lax.rsqrt(squares / D + EPSILON)
    hidden = (jax.nn.silu(gate_up[:, :ff]) * gate_up[:, ff:]).astype(bf16)

    other = swap(hidden)
    hidden = jnp.where(
        core == 0,
        jnp.concatenate([hidden, other], axis=1),
        jnp.concatenate([other, hidden], axis=1),
    )
    hidden = lax.optimization_barrier(hidden)
    first = jnp.dot(hidden, down_first, preferred_element_type=f32).astype(bf16)
    part_above = lax.optimization_barrier(jnp.dot(hidden, down_above, preferred_element_type=f32))
    part_below = lax.optimization_barrier(jnp.dot(hidden, down_below, preferred_element_type=f32))
    column = lambda a, i: a[:, i * width : (i + 1) * width]
    nothing = jnp.zeros((half, width), bf16)
    above = jnp.concatenate([y_step(first[:half], 1), nothing], axis=0)
    below = jnp.concatenate([nothing, y_step(first[half:], -1)], axis=0)
    for i in range(3):
        above = y_step((above.astype(f32) + column(part_above, i)).astype(bf16), 1)
        below = y_step((below.astype(f32) + column(part_below, i)).astype(bf16), -1)
    expert_out = column(part_below, 3) + above.astype(f32) + below.astype(f32)
    expert_out = expert_out.astype(bf16).reshape(SP, capacity, width)

    returned = exchange(expert_out, "sp").reshape(slots, width)
    combine = group_weight[:, None] * route_prob / jnp.sum(route_prob, axis=-1, keepdims=True)
    final = mixed.astype(f32)
    for k in range(TOP):
        picked = jnp.dot(select[k], returned, preferred_element_type=f32)
        final = final + combine[:, k : k + 1] * picked
    return final.astype(bf16)


def solution(mesh):
    return jax.shard_map(
        body,
        mesh=mesh,
        in_specs=(
            P("sp", "tp"),
            P("sp", None),
            P("sp", None),
            P(),
            P(None, "tp"),
            P(None, "tp"),
            P("sp", "tp"),
            P(),
            P("sp", None),
            P("sp", None),
            P("sp"),
            P("sp", None, "tp"),
            P("sp", None, "tp"),
            P("sp", None, "tp"),
        ),
        out_specs=P("sp", "tp"),
        check_vma=False,
    )
```
